256 devices in a mesh: sp: 64 (over z, x, core), tp: 4 (over y).
Axes of the slice: x: 4, y: 4, z: 8, core: 2. Of those that a mesh axis runs over, the one named last changes fastest.
Arguments:
- residual: bfloat16 [16384, 2048], P('sp', 'tp'), may hold values from -8 to 8
- query_latent: bfloat16 [16384, 512], P('sp'), may hold values from -6 to 6
- shared_latent: bfloat16 [16384, 256], P('sp'), may hold values from -6 to 6
- rotary_key: bfloat16 [16384, 32], P('sp'), may hold values from -300 to 300
- query_gain: float32 [512], replicated, may hold values from 0.1 to 1.9
- latent_gain: float32 [256], replicated, may hold values from 0.1 to 1.9
- query_narrow: bfloat16 [512, 384], P(None, 'tp'), may hold values from -0.5 to 0.5
- key_narrow: bfloat16 [256, 256], P(None, 'tp'), may hold values from -0.375 to 0.375
- value_narrow: bfloat16 [256, 256], P(None, 'tp'), may hold values from -0.375 to 0.375
- query_wide: bfloat16 [512, 640], P(None, 'tp'), may hold values from -0.5 to 0.5
- key_wide: bfloat16 [256, 512], P(None, 'tp'), may hold values from -0.375 to 0.375
- value_wide: bfloat16 [256, 512], P(None, 'tp'), may hold values from -0.375 to 0.375
- output_narrow: bfloat16 [256, 2048], P('tp'), may hold values from -1.75 to 1.75
- output_wide: bfloat16 [512, 2048], P('tp'), may hold values from -1.75 to 1.75
- first_gain: float32 [2048], P('tp'), may hold values from 0.1 to 1.9
- first_bias: float32 [2048], P('tp'), may hold values from -1.5 to 1.5
- gate_weight: bfloat16 [2048, 5632], P('sp', 'tp'), may hold values from -0.125 to 0.125
- up_weight: bfloat16 [2048, 5632], P('sp', 'tp'), may hold values from -0.125 to 0.125
- down_weight: bfloat16 [5632, 2048], P('tp', 'sp'), may hold values from -0.078125 to 0.078125
- second_gain: float32 [2048], P('tp'), may hold values from 0.1 to 1.9
- second_bias: float32 [2048], P('tp'), may hold values from -1.5 to 1.5
Outputs:
- layer_out: bfloat16 [16384, 2048], P('sp', 'tp')
The draws below stay inside these ranges and needn't reach their ends.
All inputs are finite; a program needn't handle non-finite values.
Results may differ from the reference program's by a relative error of at most 0.017.
The reference program's roundings to bfloat16 on the way count: a program that leaves them out, or rounds other values in their place, can miss the bound.
Values may be sent and summed in bfloat16 or wider, within the bound.
A program may use at most 192 MiB of HBM per device.

```python
import math
import jax
import jax.numpy as jnp
from jax import lax

D = 2048
FF = 5632
QL = 512
KVL = 256
ROPE = 32
HEADS_A = 4
HEADS_B = 4
NOPE_A = 64
V_A = 64
NOPE_B = 128
V_B = 128
GRID_W = 64
TOKENS = 16384


def draw_residual(key, part):
    col_scale = jnp.exp(jnp.linspace(math.log(0.5), math.log(1.5), D))
    base = jax.random.normal(key, (TOKENS, D), dtype=jnp.float32) * col_scale
    return jnp.clip(base, -8.0, 8.0).astype(jnp.bfloat16)


def draw_rotary_key(key, part):
    base = jax.random.normal(key, (TOKENS, ROPE), dtype=jnp.float32)
    return jnp.clip(base, -300.0, 300.0).astype(jnp.bfloat16)


def block_levels(stream_key, shape, cuts, least, high):
    level = 1.0
    for dim, blocks in cuts:
        steps = jax.random.uniform(jax.random.fold_in(jax.random.fold_in(stream_key, 6), dim), (blocks,), jnp.float32, least / len(cuts), high / len(cuts))
        level = level * jnp.repeat(jnp.exp(steps), shape[dim] // blocks).reshape((-1,) + (1,) * (len(shape) - 1 - dim))
    return level


def bell_draw(rng, dims, scale, most, shards=(), kind=jnp.bfloat16):
    result = scale * jax.random.normal(rng, dims, jnp.float32)
    if shards:
        result = result * block_levels(rng, dims, shards, -0.22, 0.18)
    return jnp.clip(result, -most, most).astype(kind)


def setup_inputs(seed: int = 0) -> dict:
    seeds = jax.random.split(jax.random.key(seed), 22)
    return {
        "residual": draw_residual(jax.random.fold_in(seeds[21], 71), 0),
        "query_latent": bell_draw(seeds[1], (TOKENS, QL), 1.0, 6.0, ((0, 64),)),
        "shared_latent": bell_draw(seeds[2], (TOKENS, KVL), 1.0, 6.0, ((0, 64),)),
        "rotary_key": draw_rotary_key(jax.random.fold_in(seeds[21], 71), 0),
        "query_gain": jnp.clip(1.0 + 0.18 * jax.random.normal(seeds[4], (QL,), jnp.float32), 0.1, 1.9),
        "latent_gain": jnp.clip(1.0 + 0.18 * jax.random.normal(seeds[5], (KVL,), jnp.float32), 0.1, 1.9),
        "query_narrow": bell_draw(seeds[6], (QL, HEADS_A * (NOPE_A + ROPE)), (QL // 4) ** -0.5, 0.5, ((1, 4),)),
        "key_narrow": bell_draw(seeds[7], (KVL, HEADS_A * NOPE_A), KVL ** -0.5, 0.375, ((1, 4),)),
        "value_narrow": bell_draw(seeds[8], (KVL, HEADS_A * V_A), KVL ** -0.5, 0.375, ((1, 4),)),
        "query_wide": bell_draw(seeds[9], (QL, HEADS_B * (NOPE_B + ROPE)), (QL // 4) ** -0.5, 0.5, ((1, 4),)),
        "key_wide": bell_draw(seeds[10], (KVL, HEADS_B * NOPE_B), KVL ** -0.5, 0.375, ((1, 4),)),
        "value_wide": bell_draw(seeds[11], (KVL, HEADS_B * V_B), KVL ** -0.5, 0.375, ((1, 4),)),
        "output_narrow": bell_draw(seeds[12], (HEADS_A * V_A, D), ((HEADS_A * V_A + HEADS_B * V_B) // 64) ** -0.5, 1.75, ((0, 4),)),
        "output_wide": bell_draw(seeds[13], (HEADS_B * V_B, D), ((HEADS_A * V_A + HEADS_B * V_B) // 64) ** -0.5, 1.75, ((0, 4),)),
        "first_gain": jnp.clip(1.0 + 0.18 * jax.random.normal(seeds[14], (D,), jnp.float32), 0.1, 1.9),
        "first_bias": bell_draw(seeds[15], (D,), 0.3, 1.5, ((0, 4),), jnp.float32),
        "gate_weight": bell_draw(seeds[16], (D, FF), D ** -0.5, 0.125, ((0, 64), (1, 4))),
        "up_weight": bell_draw(seeds[17], (D, FF), D ** -0.5, 0.125, ((0, 64), (1, 4))),
        "down_weight": bell_draw(seeds[18], (FF, D), FF ** -0.5, 0.078125, ((0, 4), (1, 64))),
        "second_gain": jnp.clip(1.0 + 0.18 * jax.random.normal(seeds[19], (D,), jnp.float32), 0.1, 1.9),
        "second_bias": bell_draw(seeds[20], (D,), 0.3, 1.5, ((0, 4),), jnp.float32),
    }


EPS_ROOT = 1e-06
EPS_LAYER = 1e-05
THETA = 10000.0
DEEP_ALPHA = 2.0 ** 0.25

def rotate(half_part, angle):
    lower, upper = jnp.split(half_part, 2, axis=-1)
    cosine = jnp.cos(angle)
    sine = jnp.sin(angle)
    return jnp.concatenate([lower * cosine - upper * sine, upper * cosine + lower * sine], axis=-1)

def turn_axial(values_in, positions):
    quarter = values_in.shape[-1] // 4
    freqs = THETA ** (-(2.0 * jnp.arange(quarter, dtype=jnp.float32)) / (2 * quarter))
    row_angle = (positions // GRID_W).astype(jnp.float32)[:, None, None] * freqs
    col_angle = (positions % GRID_W).astype(jnp.float32)[:, None, None] * freqs
    first_half, second_half = jnp.split(values_in, 2, axis=-1)
    return jnp.concatenate([rotate(first_half, row_angle), rotate(second_half, col_angle)], axis=-1)

def root_scale(latent, gain):
    floated = latent.astype(jnp.float32)
    return floated * lax.rsqrt(lax.optimization_barrier(jnp.mean(floated * floated, axis=-1, keepdims=True)) + EPS_ROOT) * gain.astype(jnp.float32)

def make_query(normed, weight, plain_dim, positions):
    product = jnp.dot(normed, weight, preferred_element_type=jnp.float32)
    head_count = weight.shape[1] // (plain_dim + ROPE)
    product = product.reshape(product.shape[0], head_count, plain_dim + ROPE)
    turned = turn_axial(product[:, :, plain_dim:], positions)
    return jnp.concatenate([product[:, :, :plain_dim], turned], axis=-1).astype(jnp.bfloat16)

def attend(queries, key_rows, value_rows, rotary_rows, plain_dim):
    count, head_count, query_dim = queries.shape
    block_size = math.gcd(count, 512)
    score_scale = query_dim ** (-0.5)
    key_float = key_rows.astype(jnp.float32)
    value_float = value_rows.astype(jnp.float32)
    rotary_float = rotary_rows.astype(jnp.float32)

    def per_block(query_block):
        query_float = query_block.astype(jnp.float32)
        scores = jnp.einsum('qhd,khd->hqk', query_float[:, :, :plain_dim], key_float)
        scores = (scores + jnp.einsum('qhd,kd->hqk', query_float[:, :, plain_dim:], rotary_float)) * score_scale
        largest = lax.optimization_barrier(jnp.max(scores, axis=-1, keepdims=True))
        raised = jnp.exp(scores - largest)
        totals = lax.optimization_barrier(jnp.sum(raised, axis=-1))
        rounded = lax.optimization_barrier(raised.astype(jnp.bfloat16)).astype(jnp.float32)
        output = jnp.einsum('hqk,khd->qhd', rounded, value_float) / totals.T[:, :, None]
        return output.astype(jnp.bfloat16)
    blocks = lax.map(per_block, queries.reshape(count // block_size, block_size, head_count, query_dim))
    return blocks.reshape(count, head_count * value_rows.shape[2])

def layer_norm(summed, gain, bias):
    center = lax.optimization_barrier(jnp.mean(summed, axis=-1, keepdims=True))
    spread = lax.optimization_barrier(jnp.mean((summed - center) * (summed - center), axis=-1, keepdims=True))
    normed = (summed - center) * lax.rsqrt(spread + EPS_LAYER) * gain.astype(jnp.float32) + bias.astype(jnp.float32)
    return normed.astype(jnp.bfloat16)

def reference(residual, query_latent, shared_latent, rotary_key, query_gain, latent_gain, query_narrow, key_narrow, value_narrow, query_wide, key_wide, value_wide, output_narrow, output_wide, first_gain, first_bias, gate_weight, up_weight, down_weight, second_gain, second_bias):
    positions = jnp.arange(residual.shape[0], dtype=jnp.int32)
    query_normed = root_scale(query_latent, query_gain).astype(jnp.bfloat16)
    latent_normed = root_scale(shared_latent, latent_gain).astype(jnp.bfloat16)
    rotary_rows = turn_axial(rotary_key.astype(jnp.float32)[:, None, :], positions)[:, 0, :].astype(jnp.bfloat16)

    def group(query_weight, key_weight, value_weight, plain_dim, value_dim):
        queries = make_query(query_normed, query_weight, plain_dim, positions)
        head_count = queries.shape[1]
        key_rows = jnp.dot(latent_normed, key_weight, preferred_element_type=jnp.float32).astype(jnp.bfloat16)
        value_rows = jnp.dot(latent_normed, value_weight, preferred_element_type=jnp.float32).astype(jnp.bfloat16)
        key_rows = key_rows.reshape(key_rows.shape[0], head_count, plain_dim)
        value_rows = value_rows.reshape(value_rows.shape[0], head_count, value_dim)
        return attend(queries, key_rows, value_rows, rotary_rows, plain_dim)
    attended_narrow = group(query_narrow, key_narrow, value_narrow, NOPE_A, V_A)
    attended_wide = group(query_wide, key_wide, value_wide, NOPE_B, V_B)
    mixed = jnp.dot(attended_narrow, output_narrow, preferred_element_type=jnp.float32)
    mixed = mixed + jnp.dot(attended_wide, output_wide, preferred_element_type=jnp.float32)
    normed_first = layer_norm(DEEP_ALPHA * residual.astype(jnp.float32) + mixed, first_gain, first_bias)
    gate = jnp.dot(normed_first, gate_weight, preferred_element_type=jnp.float32)
    lifted = jnp.dot(normed_first, up_weight, preferred_element_type=jnp.float32)
    hidden = (jax.nn.silu(gate) * lifted).astype(jnp.bfloat16)
    feed = jnp.dot(hidden, down_weight, preferred_element_type=jnp.float32)
    return layer_norm(DEEP_ALPHA * normed_first.astype(jnp.float32) + feed, second_gain, second_bias)
```

```python
import jax
import jax.numpy as jnp
from jax import lax
from jax.experimental import pallas as pl
from jax.experimental.pallas import tpu as pltpu
from jax.sharding import PartitionSpec as P

ROPE = 32
NOPE_A = 64
V_A = 64
NOPE_B = 128
V_B = 128
GRID_W = 64
EPS_ROOT = 1e-06
EPS_LAYER = 1e-05
THETA = 10000.0
DEEP_ALPHA = 2.0**0.25
LOG2E = 1.4426950408889634

NZ, NX, NY = 8, 4, 4
ROWS = 256
LAT = 256
DW = 512
D = 2048
FH = 1408
WB = 2 * FH
WA = FH
SLOT = 32
VD = V_A + V_B
KX = 128 + 256
C_A = (NOPE_A + ROPE) ** -0.5 * LOG2E
C_B = (NOPE_B + ROPE) ** -0.5 * LOG2E
MESH = pl.DeviceIdType.MESH
F32, BF16 = jnp.float32, jnp.bfloat16


def numbered(**counts):
    at, table = 0, {}
    for name, count in counts.items():
        table[name] = at
        at += count
    return table, at


M, MESSAGES = numbered(
    Q=6, KM=5, KP=4, KT=8, A1=4, AM=5, AP=4, BM=5, BP=4, XP=8, XM=8, RL=8, PW=8, O=4, OS=4,
    WO=6, AT=4, S1=4, G=5, F=4, S2=4,
)


def dot(a, b, dims):
    return lax.dot_general(a, b, (dims, ((), ())), preferred_element_type=F32)


def root_scale(latent, gain):
    x = latent.astype(F32)
    return x * lax.rsqrt(jnp.mean(x * x, axis=-1, keepdims=True) + EPS_ROOT) * gain


def turn(v, tab):
    cr, sr, cc, sc = tab[0:8], tab[8:16], tab[16:24], tab[24:32]
    a, b, c, d = v[0:8], v[8:16], v[16:24], v[24:32]
    return jnp.concatenate([a * cr - b * sr, b * cr + a * sr, c * cc - d * sc, d * cc + c * sc], axis=0)


def layer_kernel(
    res_ref, ql_ref, sl_ref, rk_ref, qg_ref, lg_ref, wqn_ref, kn_ref, vn_ref, wqw_ref, kw_ref,
    vw_ref, on_ref, ow_ref, g1_ref, b1_ref, gate_ref, up_ref, down_ref, g2_ref, b2_ref, tab_ref,
    out_ref,
    kvbuf, qbuf, wbuf, wk, wv, kx, vx, ml, acc, osend, orecv, srecv, att, wo, st1, sr1, st2, sr2,
    xbuf, gbuf, hid, fsend, frecv, hres, ss, rs, ls,
):
    s, t = lax.axis_index("sp"), lax.axis_index("tp")
    c = lax.rem(s, 2)
    x = lax.rem(lax.div(s, 2), NX)
    z = lax.div(s, 2 * NX)

    def at_z(off):
        return lax.rem(z + off + NZ, NZ)

    def at_x(off):
        return lax.rem(x + off + NX, NX)

    def at_y(off):
        return lax.rem(t + off + NY, NY)

    def dev_z(off):
        return (at_z(off) * (2 * NX) + x * 2 + c, t)

    def dev_x(off):
        return (z * (2 * NX) + at_x(off) * 2 + c, t)

    def dev_y(off):
        return (s, at_y(off))

    partner = (s + 1 - 2 * c, t)
    zz = lambda u: at_z(-u) if u <= 3 else at_z(u - 3)

    def msg(src, dst, i, dev):
        return pltpu.make_async_remote_copy(
            src_ref=src, dst_ref=dst, send_sem=ss.at[i], recv_sem=rs.at[i],
            device_id=dev, device_id_type=MESH,
        )

    def send(src, dst, i, dev):
        msg(src, dst, i, dev).start()

    def arrived(dst, i):
        msg(dst, dst, i, partner).wait_recv()

    def sent(src, i):
        msg(src, src, i, partner).wait_send()

    b_slot = lambda zi, xi: wbuf.at[zi, xi, c, :, 0:WB]
    a_slot = lambda zi, xi: wbuf.at[zi, xi, c, :, WB : WB + WA]
    a_row = lambda zi: wbuf.at[zi, :, c, :, WB : WB + WA]

    own = [
        pltpu.make_async_copy(gate_ref, wbuf.at[z, x, c, :, 0:FH], ls.at[0]),
        pltpu.make_async_copy(up_ref, wbuf.at[z, x, c, :, FH:WB], ls.at[1]),
        pltpu.make_async_copy(down_ref, wbuf.at[z, x, c, :, WB : WB + WA], ls.at[2]),
        pltpu.make_async_copy(on_ref.at[:, pl.ds(pl.multiple_of(t * DW, DW), DW)], wo.at[t, 0:V_A, :], ls.at[3]),
        pltpu.make_async_copy(ow_ref.at[:, pl.ds(pl.multiple_of(t * DW, DW), DW)], wo.at[t, V_A:VD, :], ls.at[4]),
    ]
    for o in own:
        o.start()

    barrier = pltpu.get_barrier_semaphore()
    friends = [dev_z(1), dev_z(-1), dev_x(1), dev_x(2), dev_x(3), partner, dev_y(1), dev_y(2), dev_y(3)]
    for f in friends:
        pl.semaphore_signal(barrier, inc=1, device_id=f, device_id_type=MESH)

    tab = tab_ref[...]
    kvbuf[z, c, 0:ROWS, :] = root_scale(sl_ref[...], lg_ref[...]).astype(BF16)
    kvbuf[z, c, ROWS : ROWS + ROPE, :] = turn(rk_ref[...].astype(F32), tab).astype(BF16)
    qn = root_scale(ql_ref[...], qg_ref[...]).astype(BF16)
    narrow = dot(wqn_ref[...], qn, ((1,), (1,)))
    wide = dot(wqw_ref[...], qn, ((1,), (1,)))
    qbuf[x, 0:96, :] = jnp.concatenate([narrow[0:NOPE_A], turn(narrow[NOPE_A:], tab)], axis=0).astype(BF16)
    qbuf[x, 224:384, :] = jnp.concatenate([turn(wide[NOPE_B:], tab), wide[0:NOPE_B]], axis=0).astype(BF16)
    for j in range(NX):
        qbuf[j, 96:224, :] = jnp.zeros((128, ROWS), BF16)
    wk[:, 0:64] = kn_ref[...]
    wk[:, 64:128] = jnp.zeros((LAT, 64), BF16)
    wk[:, 128:256] = kw_ref[...]
    wv[0:V_A, :] = vn_ref[...]
    wv[V_A:VD, :] = vw_ref[...]

    pl.semaphore_wait(barrier, len(friends))

    send(kvbuf.at[z, c], kvbuf.at[z, c], M["KM"] + 1, dev_z(-1))
    send(kvbuf.at[z, c], kvbuf.at[z, c], M["KP"] + 1, dev_z(1))
    send(kvbuf.at[z, c], kvbuf.at[z, c], M["KT"], partner)
    for j in (2, 1, 3):
        for half, rows in enumerate((slice(0, 96), slice(224, 384))):
            send(qbuf.at[x, rows, :], qbuf.at[x, rows, :], M["Q"] + (j - 1) * 2 + half, dev_x(j))
    for o in own[:3]:
        o.wait()
    for j in (2, 1, 3):
        send(a_slot(z, x), a_slot(z, x), M["A1"] + j, dev_x(j))
    send(b_slot(z, x), b_slot(z, x), M["BM"] + 1, dev_z(-1))
    send(b_slot(z, x), b_slot(z, x), M["BP"] + 1, dev_z(1))
    send(b_slot(z, x), b_slot(z, x), M["XP"], dev_x(1))
    send(b_slot(z, x), b_slot(z, x), M["XM"], dev_x(-1))
    for j in (2, 1, 3):
        cols = pl.ds(pl.multiple_of(at_y(j) * DW, DW), DW)
        send(on_ref.at[:, cols], wo.at[t, 0:V_A, :], M["WO"] + (j - 1) * 2, dev_y(j))
        send(ow_ref.at[:, cols], wo.at[t, V_A:VD, :], M["WO"] + (j - 1) * 2 + 1, dev_y(j))

    for j in range(NX):
        ml[j] = jnp.concatenate([jnp.full((2, ROWS), -jnp.inf, F32), jnp.zeros((6, ROWS), F32)], axis=0)
        acc[j] = jnp.zeros((VD, ROWS), F32)

    def keys_of(zs):
        lane = lax.broadcasted_iota(jnp.int32, (ROWS, 128), 1)
        for core in range(2):
            latent = kvbuf[zs, core, 0:ROWS, :]
            turned = kvbuf[zs, core, ROWS : ROWS + ROPE, :].astype(F32)
            rot = jnp.concatenate([jnp.zeros((64, ROWS), F32), turned, turned], axis=0).T
            keys = dot(latent, wk[...], ((1,), (0,)))
            at = slice(core * ROWS, (core + 1) * ROWS)
            kx[at, 0:128] = jnp.where(lane < 64, keys[:, 0:128], rot).astype(BF16)
            kx[at, 128:256] = rot.astype(BF16)
            kx[at, 256:384] = keys[:, 128:256].astype(BF16)
            vx[:, at] = dot(wv[...], latent, ((1,), (1,))).astype(BF16)

    def attend(zs):
        keys_of(zs)

        def per_rows(j, carry):
            for h, (lo, hi, vlo, vhi, scale) in enumerate(((0, 128, 0, V_A, C_A), (128, 384, V_A, VD, C_B))):
                scores = dot(kx[:, lo:hi], qbuf[j, lo:hi, :], ((1,), (0,)))
                old = ml[j, h : h + 1, :]
                new = jnp.maximum(old, jnp.max(scores, axis=0, keepdims=True))
                factor = jnp.exp2((old - new) * scale)
                raised = jnp.exp2((scores - new) * scale)
                ml[j, h : h + 1, :] = new
                ml[j, 2 + h : 3 + h, :] = ml[j, 2 + h : 3 + h, :] * factor + jnp.sum(raised, axis=0, keepdims=True)
                acc[j, vlo:vhi, :] = acc[j, vlo:vhi, :] * factor + dot(vx[vlo:vhi, :], raised.astype(BF16), ((1,), (0,)))
            return carry

        lax.fori_loop(0, NX, per_rows, 0)

    def step(k, carry):
        d = k + 1
        up_slot, low_slot = at_z(d), at_z(-d)
        arrived(kvbuf.at[up_slot, c], M["KM"] + d)

        @pl.when(d < 4)
        def _():
            send(kvbuf.at[up_slot, c], kvbuf.at[up_slot, c], M["KM"] + d + 1, dev_z(-1))

        send(kvbuf.at[up_slot, c], kvbuf.at[up_slot, c], M["KT"] + 3 + d, partner)

        @pl.when(d < 4)
        def _():
            arrived(kvbuf.at[low_slot, c], M["KP"] + d)

            @pl.when(d < 3)
            def _():
                send(kvbuf.at[low_slot, c], kvbuf.at[low_slot, c], M["KP"] + d + 1, dev_z(1))

            send(kvbuf.at[low_slot, c], kvbuf.at[low_slot, c], M["KT"] + d, partner)

        @pl.when(k == 0)
        def _():
            for j in range(1, NX):
                arrived(a_slot(z, at_x(-j)), M["A1"] + j)
            send(a_row(z), a_row(z), M["AM"] + 1, dev_z(-1))
            send(a_row(z), a_row(z), M["AP"] + 1, dev_z(1))
            for j in range(1, NX):
                for half, rows in enumerate((slice(0, 96), slice(224, 384))):
                    arrived(qbuf.at[at_x(-j), rows, :], M["Q"] + (j - 1) * 2 + half)

        arrived(kvbuf.at[at_z(-k), 1 - c], M["KT"] + k)
        attend(at_z(-k))

        arrived(b_slot(up_slot, x), M["BM"] + d)

        @pl.when(d < 4)
        def _():
            send(b_slot(up_slot, x), b_slot(up_slot, x), M["BM"] + d + 1, dev_z(-1))

        send(b_slot(up_slot, x), b_slot(up_slot, x), M["XP"] + 3 + d, dev_x(1))
        send(b_slot(up_slot, x), b_slot(up_slot, x), M["XM"] + 3 + d, dev_x(-1))

        @pl.when(d < 4)
        def _():
            arrived(b_slot(low_slot, x), M["BP"] + d)

            @pl.when(d < 3)
            def _():
                send(b_slot(low_slot, x), b_slot(low_slot, x), M["BP"] + d + 1, dev_z(1))

            send(b_slot(low_slot, x), b_slot(low_slot, x), M["XP"] + d, dev_x(1))
            send(b_slot(low_slot, x), b_slot(low_slot, x), M["XM"] + d, dev_x(-1))

        @pl.when(k > 0)
        def _():
            arrived(a_row(at_z(k)), M["AM"] + k)
            send(a_row(at_z(k)), a_row(at_z(k)), M["AM"] + k + 1, dev_z(-1))
            arrived(a_row(at_z(-k)), M["AP"] + k)

            @pl.when(k < 3)
            def _():
                send(a_row(at_z(-k)), a_row(at_z(-k)), M["AP"] + k + 1, dev_z(1))

        arrived(kvbuf.at[at_z(d), 1 - c], M["KT"] + 4 + k)
        attend(at_z(d))
        return carry

    lax.fori_loop(0, 4, step, 0)

    for j in range(NX):
        for h, (vlo, vhi) in enumerate(((0, V_A), (V_A, VD))):
            osend[j, vlo:vhi, :] = (acc[j, vlo:vhi, :] / ml[j, 2 + h : 3 + h, :]).astype(BF16)
    for j in (2, 1, 3):
        send(osend.at[at_x(j)], orecv.at[j - 1], M["O"] + j, dev_x(j))
        send(ml.at[at_x(j)], srecv.at[j - 1], M["OS"] + j, dev_x(j))

    def relay(u):
        zu = zz(u)
        arrived(b_slot(zu, at_x(-1)), M["XP"] + u)
        if u <= 3:
            send(b_slot(zu, at_x(-1)), b_slot(zu, at_x(-1)), M["RL"] + u, dev_x(1))
        arrived(b_slot(zu, at_x(1)), M["XM"] + u)
        if u > 3:
            send(b_slot(zu, at_x(1)), b_slot(zu, at_x(1)), M["RL"] + u, dev_x(-1))

    def across(u):
        arrived(b_slot(zz(u), at_x(2)), M["RL"] + u)
        send(wbuf.at[zz(u), :, c], wbuf.at[zz(u), :, c], M["PW"] + u, partner)

    for u in (0, 1, 4, 2, 5):
        relay(u)

    for j in range(1, NX):
        arrived(orecv.at[j - 1], M["O"] + j)
        arrived(srecv.at[j - 1], M["OS"] + j)
    for h, (vlo, vhi, scale) in enumerate(((0, V_A, C_A), (V_A, VD, C_B))):
        tops = [ml[x, h : h + 1, :]] + [srecv[j, h : h + 1, :] for j in range(3)]
        sums = [ml[x, 2 + h : 3 + h, :]] + [srecv[j, 2 + h : 3 + h, :] for j in range(3)]
        parts = [osend[x, vlo:vhi, :]] + [orecv[j, vlo:vhi, :] for j in range(3)]
        top = jnp.maximum(jnp.maximum(tops[0], tops[1]), jnp.maximum(tops[2], tops[3]))
        shares = [total * jnp.exp2((m - top) * scale) for m, total in zip(tops, sums)]
        total = shares[0] + shares[1] + shares[2] + shares[3]
        mixed = sum(part.astype(F32) * (share / total) for part, share in zip(parts, shares))
        att[t, vlo:vhi, :] = mixed.astype(BF16)
    for j in (2, 1, 3):
        send(att.at[t], att.at[t], M["AT"] + j, dev_y(j))

    for u in (3, 6, 7):
        relay(u)
    arrived(a_row(at_z(4)), M["AM"] + 4)
    for u in (0, 1, 4):
        across(u)

    for o in own[3:]:
        o.wait()
    for j in range(1, NY):
        for half, rows in enumerate((slice(0, V_A), slice(V_A, VD))):
            arrived(wo.at[at_y(-j), rows, :], M["WO"] + (j - 1) * 2 + half)
    for j in range(1, NY):
        arrived(att.at[at_y(-j)], M["AT"] + j)

    def norm(stat, got, first, gain_ref, bias_ref):
        h = hres[...]
        center = jnp.mean(h, axis=1, keepdims=True)
        apart = jnp.sum((h - center) * (h - center), axis=1, keepdims=True)
        lane = lax.broadcasted_iota(jnp.int32, (ROWS, 128), 1)
        both = jnp.where(lane == 0, center, jnp.where(lane == 1, apart, 0.0))
        stat[...] = both.T[0:8]
        for j in (2, 1, 3):
            send(stat, got.at[j - 1], first + j, dev_y(j))
        for j in range(1, NY):
            arrived(got.at[j - 1], first + j)
        centers = [stat[0:1, :]] + [got[j, 0:1, :] for j in range(3)]
        aparts = [stat[1:2, :]] + [got[j, 1:2, :] for j in range(3)]
        middle = (centers[0] + centers[1] + centers[2] + centers[3]) * 0.25
        spread = sum(aparts) + DW * sum((m - middle) * (m - middle) for m in centers)
        root = lax.rsqrt(spread * (1.0 / D) + EPS_LAYER)
        cols = jnp.concatenate([middle, root, jnp.zeros((126, ROWS), F32)], axis=0).T
        return ((h - cols[:, 0:1]) * cols[:, 1:2] * gain_ref[...] + bias_ref[...]).astype(BF16)

    mixed = dot(att[...].reshape(NY * VD, ROWS), wo[...].reshape(NY * VD, DW), ((0,), (0,)))
    hres[...] = DEEP_ALPHA * res_ref[...].astype(F32) + mixed
    mine = pl.ds(pl.multiple_of(t * DW, DW), DW)
    normed = norm(st1, sr1, M["S1"], g1_ref, b1_ref)
    xbuf[:, mine] = normed
    hres[...] = DEEP_ALPHA * normed.astype(F32)

    x_part = lambda off, rows: xbuf.at[rows, pl.ds(pl.multiple_of(at_y(off) * DW, DW), DW)]
    every, first_half, second_half = slice(0, ROWS), slice(0, ROWS // 2), slice(ROWS // 2, ROWS)
    send(x_part(0, every), x_part(0, every), M["G"] + 1, dev_y(1))
    send(x_part(0, every), x_part(0, every), M["G"] + 2, dev_y(-1))
    for u in (2, 5):
        across(u)
    arrived(x_part(-1, every), M["G"] + 1)
    send(x_part(-1, first_half), x_part(-1, first_half), M["G"] + 3, dev_y(1))
    arrived(x_part(1, every), M["G"] + 2)
    send(x_part(1, second_half), x_part(1, second_half), M["G"] + 4, dev_y(-1))
    for u in (3, 6, 7):
        across(u)
    arrived(x_part(2, first_half), M["G"] + 3)
    arrived(x_part(2, second_half), M["G"] + 4)
    for u in range(NZ):
        arrived(wbuf.at[zz(u), :, 1 - c], M["PW"] + u)

    def gate_up(n, carry):
        cols = pl.ds(pl.multiple_of(n * 256, 256), 256)
        gbuf[:, cols] = dot(xbuf[...], wbuf[:, :, :, :, cols].reshape(D, 256), ((1,), (0,)))
        return carry

    lax.fori_loop(0, WB // 256, gate_up, 0)
    gate = gbuf[:, 0:FH]
    hid[...] = (gate / (1.0 + jnp.exp(-gate)) * gbuf[:, FH:WB]).astype(BF16)

    def feed(off):
        return dot(hid[...], wbuf[pl.ds(at_y(off) * 2, 2), :, :, :, WB : WB + WA].reshape(DW, FH), ((1,), (1,)))

    for j in (2, 1, 3):
        fsend[j - 1] = feed(j).astype(BF16)
        send(fsend.at[j - 1], frecv.at[j - 1], M["F"] + j, dev_y(j))
    hres[...] += feed(0)
    for j in range(1, NY):
        arrived(frecv.at[j - 1], M["F"] + j)
    hres[...] += frecv[0].astype(F32) + frecv[1].astype(F32) + frecv[2].astype(F32)
    out_ref[...] = norm(st2, sr2, M["S2"], g2_ref, b2_ref)

    for j in range(1, NX):
        sent(qbuf.at[0, 0:96, :], M["Q"] + (j - 1) * 2)
        sent(qbuf.at[0, 224:384, :], M["Q"] + (j - 1) * 2 + 1)
        sent(a_slot(0, 0), M["A1"] + j)
        sent(osend.at[0], M["O"] + j)
        sent(ml.at[0], M["OS"] + j)
        sent(wo.at[0, 0:V_A, :], M["WO"] + (j - 1) * 2)
        sent(wo.at[0, V_A:VD, :], M["WO"] + (j - 1) * 2 + 1)
        sent(att.at[0], M["AT"] + j)
        sent(st1, M["S1"] + j)
        sent(fsend.at[0], M["F"] + j)
        sent(st2, M["S2"] + j)
    for d in range(1, 5):
        for name, ref in (("K", kvbuf.at[0, 0]), ("A", a_row(0)), ("B", b_slot(0, 0))):
            sent(ref, M[name + "M"] + d)
            if d < 4:
                sent(ref, M[name + "P"] + d)
    for u in range(NZ):
        sent(kvbuf.at[0, 0], M["KT"] + u)
        sent(b_slot(0, 0), M["XP"] + u)
        sent(b_slot(0, 0), M["XM"] + u)
        sent(b_slot(0, 0), M["RL"] + u)
        sent(wbuf.at[0, :, c], M["PW"] + u)
    for i in (1, 2):
        sent(x_part(0, every), M["G"] + i)
        sent(x_part(0, first_half), M["G"] + 2 + i)


def body(
    residual, query_latent, shared_latent, rotary_key, query_gain, latent_gain, query_narrow, key_narrow,
    value_narrow, query_wide, key_wide, value_wide, output_narrow, output_wide, first_gain, first_bias,
    gate_weight, up_weight, down_weight, second_gain, second_bias,
):
    positions = lax.axis_index("sp") * ROWS + jnp.arange(ROWS, dtype=jnp.int32)
    quarter = ROPE // 4
    freqs = THETA ** (-(2.0 * jnp.arange(quarter, dtype=F32)) / (2 * quarter))
    row_angle = freqs[:, None] * (positions // GRID_W).astype(F32)[None, :]
    col_angle = freqs[:, None] * (positions % GRID_W).astype(F32)[None, :]
    tab = jnp.concatenate([jnp.cos(row_angle), jnp.sin(row_angle), jnp.cos(col_angle), jnp.sin(col_angle)], axis=0)
    row = lambda v: v.reshape(1, -1)
    operands = (
        residual, query_latent, shared_latent, rotary_key.T, row(query_gain), row(latent_gain), query_narrow.T,
        key_narrow, value_narrow.T, query_wide.T, key_wide, value_wide.T, output_narrow, output_wide,
        row(first_gain), row(first_bias), gate_weight, up_weight, down_weight.T, row(second_gain),
        row(second_bias), tab,
    )
    vmem = pl.BlockSpec(memory_space=pltpu.VMEM)
    return pl.pallas_call(
        layer_kernel,
        out_shape=jax.ShapeDtypeStruct((ROWS, DW), BF16),
        in_specs=[vmem] * len(operands),
        out_specs=vmem,
        scratch_shapes=[
            pltpu.VMEM((NZ, 2, ROWS + ROPE, LAT), BF16),
            pltpu.VMEM((NX, KX, ROWS), BF16),
            pltpu.VMEM((NZ, NX, 2, SLOT, WB + WA), BF16),
            pltpu.VMEM((LAT, 256), BF16),
            pltpu.VMEM((VD, LAT), BF16),
            pltpu.VMEM((2 * ROWS, KX), BF16),
            pltpu.VMEM((VD, 2 * ROWS), BF16),
            pltpu.VMEM((NX, 8, ROWS), F32),
            pltpu.VMEM((NX, VD, ROWS), F32),
            pltpu.VMEM((NX, VD, ROWS), BF16),
            pltpu.VMEM((3, VD, ROWS), BF16),
            pltpu.VMEM((3, 8, ROWS), F32),
            pltpu.VMEM((NY, VD, ROWS), BF16),
            pltpu.VMEM((NY, VD, DW), BF16),
            pltpu.VMEM((8, ROWS), F32),
            pltpu.VMEM((3, 8, ROWS), F32),
            pltpu.VMEM((8, ROWS), F32),
            pltpu.VMEM((3, 8, ROWS), F32),
            pltpu.VMEM((ROWS, D), BF16),
            pltpu.VMEM((ROWS, WB), F32),
            pltpu.VMEM((ROWS, FH), BF16),
            pltpu.VMEM((3, ROWS, DW), BF16),
            pltpu.VMEM((3, ROWS, DW), BF16),
            pltpu.VMEM((ROWS, DW), F32),
            pltpu.SemaphoreType.DMA((MESSAGES,)),
            pltpu.SemaphoreType.DMA((MESSAGES,)),
            pltpu.SemaphoreType.DMA((5,)),
        ],
        compiler_params=pltpu.CompilerParams(
            collective_id=0, has_side_effects=True, vmem_limit_bytes=60 * 1024 * 1024
        ),
    )(*operands)


def solution(mesh):
    return jax.shard_map(
        body,
        mesh=mesh,
        in_specs=(
            P("sp", "tp"),
            P("sp", None),
            P("sp", None),
            P("sp", None),
            P(),
            P(),
            P(None, "tp"),
            P(None, "tp"),
            P(None, "tp"),
            P(None, "tp"),
            P(None, "tp"),
            P(None, "tp"),
            P("tp", None),
            P("tp", None),
            P("tp"),
            P("tp"),
            P("sp", "tp"),
            P("sp", "tp"),
            P("tp", "sp"),
            P("tp"),
            P("tp"),
        ),
        out_specs=P("sp", "tp"),
        check_vma=False,
    )
```

```python
import jax
import jax.numpy as jnp
from jax import lax
from jax.experimental import pallas as pl
from jax.experimental.pallas import tpu as pltpu
from jax.sharding import PartitionSpec as P

ROPE = 32
NOPE_A = 64
V_A = 64
NOPE_B = 128
V_B = 128
GRID_W = 64
EPS_ROOT = 1e-06
EPS_LAYER = 1e-05
THETA = 10000.0
DEEP_ALPHA = 2.0**0.25
LOG2E = 1.4426950408889634

NZ, NX, NY = 8, 4, 4
ROWS = 256
LAT = 256
DW = 512
D = 2048
FH = 1408
GU = 2 * FH
WT = 3 * FH
WB = GU - 256
SLOT = 32
VD = V_A + V_B
KX = 128 + 256
C_A = (NOPE_A + ROPE) ** -0.5 * LOG2E
C_B = (NOPE_B + ROPE) ** -0.5 * LOG2E
MESH = pl.DeviceIdType.MESH
F32, BF16 = jnp.float32, jnp.bfloat16


def numbered(**counts):
    at, table = 0, {}
    for name, count in counts.items():
        table[name] = at
        at += count
    return table, at


M, MESSAGES = numbered(
    Q=6, KM=5, KP=4, KT=8, A1=4, AM=4, AP=5, BM=5, BP=4, XP=8, XM=8, RL=8, PB=32, PA=8, O=4, OS=4,
    WO=6, AT=4, S1=4, G=4, F=4, S2=4,
)


def dot(a, b, dims):
    return lax.dot_general(a, b, (dims, ((), ())), preferred_element_type=F32)


def root_scale(latent, gain):
    x = latent.astype(F32)
    return x * lax.rsqrt(jnp.mean(x * x, axis=-1, keepdims=True) + EPS_ROOT) * gain


def turn(v, tab):
    cr, sr, cc, sc = tab
    a, b, c, d = v[0:8], v[8:16], v[16:24], v[24:32]
    return jnp.concatenate([a * cr - b * sr, b * cr + a * sr, c * cc - d * sc, d * cc + c * sc], axis=0)


def layer_kernel(
    res_ref, ql_ref, sl_ref, rk_ref, qg_ref, lg_ref, wqn_ref, kn_ref, vn_ref, wqw_ref, kw_ref,
    vw_ref, on_ref, ow_ref, g1_ref, b1_ref, gate_ref, up_ref, down_ref, g2_ref, b2_ref, cr_ref, sr_ref, cc_ref, sc_ref,
    out_ref,
    kvbuf, qbuf, wbuf, wk, wv, kx, vx, ml, acc, osend, orecv, srecv, att, wo, st1, sr1, st2, sr2,
    xbuf, gbuf, hid, fsend, frecv, hres, ss, rs, ls,
):
    s, t = lax.axis_index("sp"), lax.axis_index("tp")
    c = lax.rem(s, 2)
    x = lax.rem(lax.div(s, 2), NX)
    z = lax.div(s, 2 * NX)

    def at_z(off):
        return lax.rem(z + off + NZ, NZ)

    def at_x(off):
        return lax.rem(x + off + NX, NX)

    def at_y(off):
        return lax.rem(t + off + NY, NY)

    def dev_z(off):
        return (at_z(off) * (2 * NX) + x * 2 + c, t)

    def dev_x(off):
        return (z * (2 * NX) + at_x(off) * 2 + c, t)

    def dev_y(off):
        return (s, at_y(off))

    partner = (s + 1 - 2 * c, t)

    def zz(u):
        return at_z(lax.div(u + 1, 2) * (1 - 2 * lax.rem(u, 2)) if not isinstance(u, int) else (u + 1) // 2 * (1 - 2 * (u % 2)))


    def msg(src, dst, i, dev):
        return pltpu.make_async_remote_copy(
            src_ref=src, dst_ref=dst, send_sem=ss.at[i], recv_sem=rs.at[i],
            device_id=dev, device_id_type=MESH,
        )

    def send(src, dst, i, dev):
        msg(src, dst, i, dev).start()

    def arrived(dst, i):
        msg(dst, dst, i, partner).wait_recv()

    def sent(src, i):
        msg(src, src, i, partner).wait_send()

    b_slot = lambda zi, xi: wbuf.at[zi, xi, c, :, 0:WB]
    a_slot = lambda zi, xi: wbuf.at[zi, xi, c, :, WB:WT]
    a_row = lambda zi: wbuf.at[zi, :, c, :, WB:WT]

    own = [
        pltpu.make_async_copy(gate_ref, wbuf.at[z, x, c, :, 0:FH], ls.at[0]),
        pltpu.make_async_copy(up_ref, wbuf.at[z, x, c, :, FH:GU], ls.at[1]),
        pltpu.make_async_copy(down_ref, wbuf.at[z, x, c, :, GU:WT], ls.at[2]),
        pltpu.make_async_copy(on_ref.at[:, pl.ds(pl.multiple_of(t * DW, DW), DW)], wo.at[t, 0:V_A, :], ls.at[3]),
        pltpu.make_async_copy(ow_ref.at[:, pl.ds(pl.multiple_of(t * DW, DW), DW)], wo.at[t, V_A:VD, :], ls.at[4]),
    ]
    for o in own:
        o.start()

    barrier = pltpu.get_barrier_semaphore()
    friends = [dev_z(1), dev_z(-1), dev_x(1), dev_x(2), dev_x(3), partner, dev_y(1), dev_y(2), dev_y(3)]
    for f in friends:
        pl.semaphore_signal(barrier, inc=1, device_id=f, device_id_type=MESH)

    tab = (cr_ref[...], sr_ref[...], cc_ref[...], sc_ref[...])
    kvbuf[z, c, 0:ROWS, :] = root_scale(sl_ref[...], lg_ref[...]).astype(BF16)
    kvbuf[z, c, ROWS : ROWS + ROPE, :] = turn(rk_ref[...].astype(F32), tab).astype(BF16)
    qn = root_scale(ql_ref[...], qg_ref[...]).astype(BF16)
    narrow = dot(wqn_ref[...], qn, ((1,), (1,)))
    wide = dot(wqw_ref[...], qn, ((1,), (1,)))
    qbuf[x, 0:96, :] = jnp.concatenate([narrow[0:NOPE_A], turn(narrow[NOPE_A:], tab)], axis=0).astype(BF16)
    qbuf[x, 224:384, :] = jnp.concatenate([turn(wide[NOPE_B:], tab), wide[0:NOPE_B]], axis=0).astype(BF16)
    for j in range(NX):
        qbuf[j, 96:224, :] = jnp.zeros((128, ROWS), BF16)
    wk[:, 0:64] = kn_ref[...].T
    wk[:, 64:128] = jnp.zeros((LAT, 64), BF16)
    wk[:, 128:256] = kw_ref[...]
    wv[0:V_A, :] = vn_ref[...]
    wv[V_A:VD, :] = vw_ref[...].T

    pl.semaphore_wait(barrier, len(friends))

    send(kvbuf.at[z, c], kvbuf.at[z, c], M["KM"] + 1, dev_z(-1))
    send(kvbuf.at[z, c], kvbuf.at[z, c], M["KP"] + 1, dev_z(1))
    send(kvbuf.at[z, c], kvbuf.at[z, c], M["KT"], partner)
    for j in (2, 1, 3):
        for half, rows in enumerate((slice(0, 96), slice(224, 384))):
            send(qbuf.at[x, rows, :], qbuf.at[x, rows, :], M["Q"] + (j - 1) * 2 + half, dev_x(j))
    for o in own[:3]:
        o.wait()
    for j in (2, 1, 3):
        send(a_slot(z, x), a_slot(z, x), M["A1"] + j, dev_x(j))
    send(b_slot(z, x), b_slot(z, x), M["BM"] + 1, dev_z(-1))
    send(b_slot(z, x), b_slot(z, x), M["BP"] + 1, dev_z(1))
    send(b_slot(z, x), b_slot(z, x), M["XP"], dev_x(1))
    send(b_slot(z, x), b_slot(z, x), M["XM"], dev_x(-1))
    send(b_slot(z, x), b_slot(z, x), M["PB"], partner)
    for j in (2, 1, 3):
        cols = pl.ds(pl.multiple_of(at_y(j) * DW, DW), DW)
        send(on_ref.at[:, cols], wo.at[t, 0:V_A, :], M["WO"] + (j - 1) * 2, dev_y(j))
        send(ow_ref.at[:, cols], wo.at[t, V_A:VD, :], M["WO"] + (j - 1) * 2 + 1, dev_y(j))

    for j in range(NX):
        ml[j] = jnp.concatenate([jnp.full((2, ROWS), -jnp.inf, F32), jnp.zeros((6, ROWS), F32)], axis=0)
        acc[j] = jnp.zeros((VD, ROWS), F32)

    def keys_of(zs):
        lane = lax.broadcasted_iota(jnp.int32, (ROWS, 128), 1)
        for core in range(2):
            latent = kvbuf[zs, core, 0:ROWS, :]
            turned = kvbuf[zs, core, ROWS : ROWS + ROPE, :].astype(F32)
            rot = jnp.concatenate([jnp.zeros((64, ROWS), F32), turned, turned], axis=0).T
            keys = dot(latent, wk[...], ((1,), (0,)))
            at = slice(core * ROWS, (core + 1) * ROWS)
            kx[at, 0:128] = jnp.where(lane < 64, keys[:, 0:128], rot).astype(BF16)
            kx[at, 128:256] = rot.astype(BF16)
            kx[at, 256:384] = keys[:, 128:256].astype(BF16)
            vx[:, at] = dot(wv[...], latent, ((1,), (1,))).astype(BF16)

    def attend(zs):
        keys_of(zs)

        heads = ((0, 128, 0, V_A, C_A), (128, 384, V_A, VD, C_B))
        every_score = [
            [dot(kx[:, lo:hi], qbuf[j, lo:hi, :], ((1,), (0,))) for lo, hi, _, _, _ in heads] for j in range(NX)
        ]
        for j in range(NX):
            for h, (_, _, vlo, vhi, scale) in enumerate(heads):
                scores = every_score[j][h]
                old = ml[j, h : h + 1, :]
                new = jnp.maximum(old, jnp.max(scores, axis=0, keepdims=True))
                factor = jnp.exp2((old - new) * scale)
                raised = jnp.exp2((scores - new) * scale)
                ml[j, h : h + 1, :] = new
                ml[j, 2 + h : 3 + h, :] = ml[j, 2 + h : 3 + h, :] * factor + jnp.sum(raised, axis=0, keepdims=True)
                acc[j, vlo:vhi, :] = acc[j, vlo:vhi, :] * factor + dot(vx[vlo:vhi, :], raised.astype(BF16), ((1,), (0,)))

    def to_partner(u, zi, way):
        xi = at_x((0, -1, 1, 2)[way])
        send(b_slot(zi, xi), b_slot(zi, xi), M["PB"] + 4 * u + way, partner)

    def row_to_partner(u, zi):
        send(a_row(zi), a_row(zi), M["PA"] + u, partner)

    def to_x(u, zi):
        send(b_slot(zi, x), b_slot(zi, x), M["XP"] + u, dev_x(1))
        send(b_slot(zi, x), b_slot(zi, x), M["XM"] + u, dev_x(-1))

    def step(k, carry):
        d = k + 1
        u1 = 2 * k - lax.div(k + 3, 4)
        low, up = 2 * d - 1, 2 * d - lax.div(d, 4)
        up_slot, low_slot = at_z(d), at_z(-d)
        arrived(kvbuf.at[up_slot, c], M["KM"] + d)

        @pl.when(d < 4)
        def _():
            send(kvbuf.at[up_slot, c], kvbuf.at[up_slot, c], M["KM"] + d + 1, dev_z(-1))

        send(kvbuf.at[up_slot, c], kvbuf.at[up_slot, c], M["KT"] + up, partner)

        @pl.when(d < 4)
        def _():
            arrived(kvbuf.at[low_slot, c], M["KP"] + d)

            @pl.when(d < 3)
            def _():
                send(kvbuf.at[low_slot, c], kvbuf.at[low_slot, c], M["KP"] + d + 1, dev_z(1))

            send(kvbuf.at[low_slot, c], kvbuf.at[low_slot, c], M["KT"] + low, partner)

        @pl.when(k == 0)
        def _():
            for j in range(1, NX):
                for half, rows in enumerate((slice(0, 96), slice(224, 384))):
                    arrived(qbuf.at[at_x(-j), rows, :], M["Q"] + (j - 1) * 2 + half)

        arrived(kvbuf.at[at_z(-k), 1 - c], M["KT"] + u1)
        attend(at_z(-k))

        arrived(b_slot(up_slot, x), M["BM"] + d)
        to_partner(up, up_slot, 0)

        @pl.when(d < 4)
        def _():
            send(b_slot(up_slot, x), b_slot(up_slot, x), M["BM"] + d + 1, dev_z(-1))

        @pl.when(d < 3)
        def _():
            to_x(up, up_slot)

        @pl.when(d < 4)
        def _():
            arrived(b_slot(low_slot, x), M["BP"] + d)
            to_partner(low, low_slot, 0)

            @pl.when(d < 3)
            def _():
                send(b_slot(low_slot, x), b_slot(low_slot, x), M["BP"] + d + 1, dev_z(1))
                to_x(low, low_slot)

        @pl.when(k == 2)
        def _():
            for j in range(1, NX):
                arrived(a_slot(z, at_x(-j)), M["A1"] + j)
            send(a_row(z), a_row(z), M["AM"] + 1, dev_z(-1))
            send(a_row(z), a_row(z), M["AP"] + 1, dev_z(1))
            row_to_partner(0, z)

        arrived(kvbuf.at[at_z(d), 1 - c], M["KT"] + up)
        attend(at_z(d))
        return carry

    lax.fori_loop(0, 4, step, 0)

    for j in range(NX):
        for h, (vlo, vhi) in enumerate(((0, V_A), (V_A, VD))):
            osend[j, vlo:vhi, :] = (acc[j, vlo:vhi, :] / ml[j, 2 + h : 3 + h, :]).astype(BF16)
    for j in (2, 1, 3):
        send(osend.at[at_x(j)], orecv.at[j - 1], M["O"] + j, dev_x(j))
        send(ml.at[at_x(j)], srecv.at[j - 1], M["OS"] + j, dev_x(j))

    for u in (5, 6, 7):
        to_x(u, zz(u))

    plus = (0, 1, 3, 5)

    def relay(u):
        zu = zz(u)
        arrived(b_slot(zu, at_x(-1)), M["XP"] + u)
        if u in plus:
            send(b_slot(zu, at_x(-1)), b_slot(zu, at_x(-1)), M["RL"] + u, dev_x(1))
        to_partner(u, zu, 1)
        arrived(b_slot(zu, at_x(1)), M["XM"] + u)
        if u not in plus:
            send(b_slot(zu, at_x(1)), b_slot(zu, at_x(1)), M["RL"] + u, dev_x(-1))
        to_partner(u, zu, 2)

    def across(u):
        arrived(b_slot(zz(u), at_x(2)), M["RL"] + u)
        to_partner(u, zz(u), 3)

    def rows_round(d):
        arrived(a_row(at_z(-d)), M["AP"] + d)
        if d < 4:
            send(a_row(at_z(-d)), a_row(at_z(-d)), M["AP"] + d + 1, dev_z(1))
        row_to_partner(2 * d - 1, at_z(-d))
        if d < 4:
            arrived(a_row(at_z(d)), M["AM"] + d)
            if d < 3:
                send(a_row(at_z(d)), a_row(at_z(d)), M["AM"] + d + 1, dev_z(-1))
            row_to_partner(2 * d, at_z(d))

    relay(0)
    relay(1)
    rows_round(1)

    for j in range(1, NX):
        arrived(orecv.at[j - 1], M["O"] + j)
        arrived(srecv.at[j - 1], M["OS"] + j)
    for h, (vlo, vhi, scale) in enumerate(((0, V_A, C_A), (V_A, VD, C_B))):
        tops = [ml[x, h : h + 1, :]] + [srecv[j, h : h + 1, :] for j in range(3)]
        sums = [ml[x, 2 + h : 3 + h, :]] + [srecv[j, 2 + h : 3 + h, :] for j in range(3)]
        parts = [osend[x, vlo:vhi, :]] + [orecv[j, vlo:vhi, :] for j in range(3)]
        top = jnp.maximum(jnp.maximum(tops[0], tops[1]), jnp.maximum(tops[2], tops[3]))
        shares = [total * jnp.exp2((m - top) * scale) for m, total in zip(tops, sums)]
        total = shares[0] + shares[1] + shares[2] + shares[3]
        mixed = sum(part.astype(F32) * (share / total) for part, share in zip(parts, shares))
        att[t, vlo:vhi, :] = mixed.astype(BF16)
    for j in (2, 1, 3):
        send(att.at[t], att.at[t], M["AT"] + j, dev_y(j))

    relay(2)
    relay(3)

    for o in own[3:]:
        o.wait()
    for j in range(1, NY):
        for half, rows in enumerate((slice(0, V_A), slice(V_A, VD))):
            arrived(wo.at[at_y(-j), rows, :], M["WO"] + (j - 1) * 2 + half)
    for j in range(1, NY):
        arrived(att.at[at_y(-j)], M["AT"] + j)

    def norm(stat, got, first, gain_ref, bias_ref, between):
        h = hres[...]
        center = jnp.mean(h, axis=1, keepdims=True)
        apart = jnp.sum((h - center) * (h - center), axis=1, keepdims=True)
        lane = lax.broadcasted_iota(jnp.int32, (ROWS, 128), 1)
        both = jnp.where(lane == 0, center, jnp.where(lane == 1, apart, 0.0))
        stat[...] = both.T[0:8]
        for j in (2, 1, 3):
            send(stat, got.at[j - 1], first + j, dev_y(j))
        between()
        for j in range(1, NY):
            arrived(got.at[j - 1], first + j)
        centers = [stat[0:1, :]] + [got[j, 0:1, :] for j in range(3)]
        aparts = [stat[1:2, :]] + [got[j, 1:2, :] for j in range(3)]
        middle = (centers[0] + centers[1] + centers[2] + centers[3]) * 0.25
        spread = sum(aparts) + DW * sum((m - middle) * (m - middle) for m in centers)
        root = lax.rsqrt(spread * (1.0 / D) + EPS_LAYER)
        cols = jnp.concatenate([middle, root, jnp.zeros((126, ROWS), F32)], axis=0).T
        return ((h - cols[:, 0:1]) * cols[:, 1:2] * gain_ref[...] + bias_ref[...]).astype(BF16)

    mixed = dot(att[...].reshape(NY * VD, ROWS), wo[...].reshape(NY * VD, DW), ((0,), (0,)))
    hres[...] = DEEP_ALPHA * res_ref[...].astype(F32) + mixed
    mine = pl.ds(pl.multiple_of(t * DW, DW), DW)
    normed = norm(st1, sr1, M["S1"], g1_ref, b1_ref, lambda: (rows_round(2), relay(4)))
    xbuf[:, mine] = normed
    hres[...] = DEEP_ALPHA * normed.astype(F32)

    x_part = lambda off: xbuf.at[:, pl.ds(pl.multiple_of(at_y(off) * DW, DW), DW)]
    for j in (2, 1, 3):
        send(x_part(0), x_part(0), M["G"] + j, dev_y(j))
    across(0)
    across(1)
    relay(5)
    across(2)
    rows_round(3)
    relay(6)
    across(3)
    relay(7)
    for j in range(1, NY):
        arrived(x_part(-j), M["G"] + j)

    def gate_up(u):
        zu = zz(u)
        features = xbuf[:, pl.ds(pl.multiple_of(zu * 256, 256), 256)]
        for n in range(WB // 256):
            cols = slice(n * 256, (n + 1) * 256)
            part = dot(features, wbuf[zu, :, :, :, cols].reshape(256, 256), ((1,), (0,)))
            gbuf[:, cols] = part if isinstance(u, int) else gbuf[:, cols] + part

    def partner_block(u):
        for way in range(4):
            arrived(wbuf.at[zz(u), at_x((0, -1, 1, 2)[way]), 1 - c, :, 0:WB], M["PB"] + 4 * u + way)

    partner_block(0)
    gate_up(0)

    def block(u, carry):
        @pl.when(u <= 4)
        def _():
            across(u + 3)

        partner_block(u)
        gate_up(u)
        return carry

    lax.fori_loop(1, NZ, block, 0)
    rows_round(4)
    for u in range(NZ):
        arrived(wbuf.at[zz(u), :, 1 - c, :, WB:WT], M["PA"] + u)
    gbuf[:, WB:GU] = dot(xbuf[...], wbuf[:, :, :, :, WB:GU].reshape(D, 256), ((1,), (0,)))
    gate = gbuf[:, 0:FH]
    hid[...] = (gate / (1.0 + jnp.exp(-gate)) * gbuf[:, FH:GU]).astype(BF16)

    def feed(off):
        return dot(hid[...], wbuf[pl.ds(at_y(off) * 2, 2), :, :, :, GU:WT].reshape(DW, FH), ((1,), (1,)))

    for j in (2, 1, 3):
        fsend[j - 1] = feed(j).astype(BF16)
        send(fsend.at[j - 1], frecv.at[j - 1], M["F"] + j, dev_y(j))
    hres[...] += feed(0)
    for j in range(1, NY):
        arrived(frecv.at[j - 1], M["F"] + j)
    hres[...] += frecv[0].astype(F32) + frecv[1].astype(F32) + frecv[2].astype(F32)
    out_ref[...] = norm(st2, sr2, M["S2"], g2_ref, b2_ref, lambda: None)

    for j in range(1, NX):
        sent(qbuf.at[0, 0:96, :], M["Q"] + (j - 1) * 2)
        sent(qbuf.at[0, 224:384, :], M["Q"] + (j - 1) * 2 + 1)
        sent(a_slot(0, 0), M["A1"] + j)
        sent(osend.at[0], M["O"] + j)
        sent(ml.at[0], M["OS"] + j)
        sent(wo.at[0, 0:V_A, :], M["WO"] + (j - 1) * 2)
        sent(wo.at[0, V_A:VD, :], M["WO"] + (j - 1) * 2 + 1)
        sent(att.at[0], M["AT"] + j)
        sent(st1, M["S1"] + j)
        sent(fsend.at[0], M["F"] + j)
        sent(st2, M["S2"] + j)
    for d in range(1, 5):
        for name, ref, last in (("K", kvbuf.at[0, 0], "M"), ("A", a_row(0), "P"), ("B", b_slot(0, 0), "M")):
            for way in "MP":
                if d < 4 or way == last:
                    sent(ref, M[name + way] + d)
    for u in range(NZ):
        sent(kvbuf.at[0, 0], M["KT"] + u)
        sent(b_slot(0, 0), M["XP"] + u)
        sent(b_slot(0, 0), M["XM"] + u)
        sent(b_slot(0, 0), M["RL"] + u)
        sent(a_row(0), M["PA"] + u)
        for way in range(4):
            sent(b_slot(0, 0), M["PB"] + 4 * u + way)
    for j in range(1, NY):
        sent(x_part(0), M["G"] + j)


def body(
    residual, query_latent, shared_latent, rotary_key, query_gain, latent_gain, query_narrow, key_narrow,
    value_narrow, query_wide, key_wide, value_wide, output_narrow, output_wide, first_gain, first_bias,
    gate_weight, up_weight, down_weight, second_gain, second_bias,
):
    positions = lax.axis_index("sp") * ROWS + jnp.arange(ROWS, dtype=jnp.int32)
    quarter = ROPE // 4
    freqs = THETA ** (-(2.0 * jnp.arange(quarter, dtype=F32)) / (2 * quarter))
    row_angle = freqs[:, None] * (positions // GRID_W).astype(F32)[None, :]
    col_angle = freqs[:, None] * (positions % GRID_W).astype(F32)[None, :]
    row = lambda v: v.reshape(1, -1)
    operands = (
        residual, query_latent, shared_latent, rotary_key.T, row(query_gain), row(latent_gain), query_narrow.T,
        key_narrow.T, value_narrow.T, query_wide.T, key_wide, value_wide, output_narrow, output_wide,
        row(first_gain), row(first_bias), gate_weight, up_weight, down_weight.T, row(second_gain),
        row(second_bias), jnp.cos(row_angle), jnp.sin(row_angle), jnp.cos(col_angle), jnp.sin(col_angle),
    )
    vmem = pl.BlockSpec(memory_space=pltpu.VMEM)
    return pl.pallas_call(
        layer_kernel,
        out_shape=jax.ShapeDtypeStruct((ROWS, DW), BF16),
        in_specs=[vmem] * len(operands),
        out_specs=vmem,
        scratch_shapes=[
            pltpu.VMEM((NZ, 2, ROWS + ROPE, LAT), BF16),
            pltpu.VMEM((NX, KX, ROWS), BF16),
            pltpu.VMEM((NZ, NX, 2, SLOT, WT), BF16),
            pltpu.VMEM((LAT, 256), BF16),
            pltpu.VMEM((VD, LAT), BF16),
            pltpu.VMEM((2 * ROWS, KX), BF16),
            pltpu.VMEM((VD, 2 * ROWS), BF16),
            pltpu.VMEM((NX, 8, ROWS), F32),
            pltpu.VMEM((NX, VD, ROWS), F32),
            pltpu.VMEM((NX, VD, ROWS), BF16),
            pltpu.VMEM((3, VD, ROWS), BF16),
            pltpu.VMEM((3, 8, ROWS), F32),
            pltpu.VMEM((NY, VD, ROWS), BF16),
            pltpu.VMEM((NY, VD, DW), BF16),
            pltpu.VMEM((8, ROWS), F32),
            pltpu.VMEM((3, 8, ROWS), F32),
            pltpu.VMEM((8, ROWS), F32),
            pltpu.VMEM((3, 8, ROWS), F32),
            pltpu.VMEM((ROWS, D), BF16),
            pltpu.VMEM((ROWS, GU), F32),
            pltpu.VMEM((ROWS, FH), BF16),
            pltpu.VMEM((3, ROWS, DW), BF16),
            pltpu.VMEM((3, ROWS, DW), BF16),
            pltpu.VMEM((ROWS, DW), F32),
            pltpu.SemaphoreType.DMA((MESSAGES,)),
            pltpu.SemaphoreType.DMA((MESSAGES,)),
            pltpu.SemaphoreType.DMA((5,)),
        ],
        compiler_params=pltpu.CompilerParams(
            collective_id=0, has_side_effects=True, vmem_limit_bytes=60 * 1024 * 1024
        ),
    )(*operands)


def solution(mesh):
    return jax.shard_map(
        body,
        mesh=mesh,
        in_specs=(
            P("sp", "tp"),
            P("sp", None),
            P("sp", None),
            P("sp", None),
            P(),
            P(),
            P(None, "tp"),
            P(None, "tp"),
            P(None, "tp"),
            P(None, "tp"),
            P(None, "tp"),
            P(None, "tp"),
            P("tp", None),
            P("tp", None),
            P("tp"),
            P("tp"),
            P("sp", "tp"),
            P("sp", "tp"),
            P("tp", "sp"),
            P("tp"),
            P("tp"),
        ),
        out_specs=P("sp", "tp"),
        check_vma=False,
    )
```

```python
import jax
import jax.numpy as jnp
from jax import lax
from jax.experimental import pallas as pl
from jax.experimental.pallas import tpu as pltpu
from jax.sharding import PartitionSpec as P

ROPE = 32
NOPE_A = 64
V_A = 64
NOPE_B = 128
V_B = 128
GRID_W = 64
EPS_ROOT = 1e-06
EPS_LAYER = 1e-05
THETA = 10000.0
DEEP_ALPHA = 2.0**0.25
LOG2E = 1.4426950408889634

NZ, NX, NY = 8, 4, 4
ROWS = 256
HALF = ROWS // 2
LAT = 256
DW = 512
D = 2048
FH = 1408
GU = 2 * FH
WT = 3 * FH
WB = GU - 256
B_COLS, A_COLS = slice(0, WB), slice(WB, WT)
SLOT = 32
VD = V_A + V_B
KX = 128 + 256
C_A = (NOPE_A + ROPE) ** -0.5 * LOG2E
C_B = (NOPE_B + ROPE) ** -0.5 * LOG2E
MESH = pl.DeviceIdType.MESH
F32, BF16 = jnp.float32, jnp.bfloat16


def numbered(**counts):
    at, table = 0, {}
    for name, count in counts.items():
        table[name] = at
        at += count
    return table, at


M, MESSAGES = numbered(
    Q=6, KZ=8, KY=24, KT=8, O=4, OS=4, WO=6, AT=4, S1=4, G=6, F=6, S2=4,
    A1=4, AM=5, AP=5, BM=5, BP=4, XP=8, XM=8, RL=8, PB=32, PA=8,
)


def dot(a, b, dims):
    return lax.dot_general(a, b, (dims, ((), ())), preferred_element_type=F32)


def root_scale(latent, gain):
    x = latent.astype(F32)
    return x * lax.rsqrt(jnp.mean(x * x, axis=-1, keepdims=True) + EPS_ROOT) * gain


def turn(v, tab):
    cr, sr, cc, sc = tab
    a, b, c, d = v[0:8], v[8:16], v[16:24], v[24:32]
    return jnp.concatenate([a * cr - b * sr, b * cr + a * sr, c * cc - d * sc, d * cc + c * sc], axis=0)


def layer_kernel(
    res_hbm, ql_hbm, sl_hbm, rk_hbm, wqn_hbm, kn_hbm, vn_hbm, wqw_hbm, kw_hbm, vw_hbm, on_ref, ow_ref,
    gate_ref, up_ref, down_ref, qg_ref, lg_ref, g1_ref, b1_ref, g2_ref, b2_ref, cr_ref, sr_ref, cc_ref, sc_ref,
    out_ref,
    res_ref, ql_ref, sl_ref, rk_ref, wqn_ref, kn_ref, vn_ref, wqw_ref, kw_ref, vw_ref,
    kvbuf, qbuf, wbuf, wk, wv, kx, vx, ml, acc, osend, orecv, srecv, att, wo, st1, sr1, st2, sr2,
    xbuf, gbuf, hid, fsend, frecv, fthru, fkeep, hres, ss, rs, ls,
):
    s, t = lax.axis_index("sp"), lax.axis_index("tp")
    c = lax.rem(s, 2)
    x = lax.rem(lax.div(s, 2), NX)
    z = lax.div(s, 2 * NX)

    def at_z(off):
        return lax.rem(z + off + NZ, NZ)

    def at_x(off):
        return lax.rem(x + off + NX, NX)

    def at_y(off):
        return lax.rem(t + off + NY, NY)

    def dev_z(off):
        return (at_z(off) * (2 * NX) + x * 2 + c, t)

    def dev_x(off):
        return (z * (2 * NX) + at_x(off) * 2 + c, t)

    def dev_y(off):
        return (s, at_y(off))

    partner = (s + 1 - 2 * c, t)

    def zz(u):
        return at_z(lax.div(u + 1, 2) * (1 - 2 * lax.rem(u, 2)) if not isinstance(u, int) else (u + 1) // 2 * (1 - 2 * (u % 2)))


    def msg(src, dst, i, dev):
        return pltpu.make_async_remote_copy(
            src_ref=src, dst_ref=dst, send_sem=ss.at[i], recv_sem=rs.at[i],
            device_id=dev, device_id_type=MESH,
        )

    def send(src, dst, i, dev):
        msg(src, dst, i, dev).start()

    def arrived(dst, i):
        msg(dst, dst, i, partner).wait_recv()

    def sent(src, i):
        msg(src, src, i, partner).wait_send()

    b_slot = lambda zi, xi: wbuf.at[zi, xi, c, :, B_COLS]
    a_slot = lambda zi, xi: wbuf.at[zi, xi, c, :, A_COLS]
    a_row = lambda zi: wbuf.at[zi, :, c, :, A_COLS]

    barrier = pltpu.get_barrier_semaphore()
    friends = [*[dev_z(off) for off in range(1, NZ)], dev_x(1), dev_x(2), dev_x(3), partner, dev_y(1), dev_y(2), dev_y(3)]
    for f in friends:
        pl.semaphore_signal(barrier, inc=1, device_id=f, device_id_type=MESH)

    my_cols = pl.ds(pl.multiple_of(t * DW, DW), DW)
    local = [
        (sl_hbm, sl_ref), (rk_hbm, rk_ref), (ql_hbm, ql_ref), (wqn_hbm, wqn_ref), (wqw_hbm, wqw_ref),
        (kn_hbm, kn_ref), (kw_hbm, kw_ref), (vn_hbm, vn_ref), (vw_hbm, vw_ref),
        (gate_ref, wbuf.at[z, x, c, :, 0:FH]), (up_ref, wbuf.at[z, x, c, :, FH:GU]),
        (down_ref, wbuf.at[z, x, c, :, GU:WT]), (on_ref.at[:, my_cols], wo.at[t, 0:V_A, :]),
        (ow_ref.at[:, my_cols], wo.at[t, V_A:VD, :]), (res_hbm, res_ref),
    ]
    local = [pltpu.make_async_copy(src, dst, ls.at[i]) for i, (src, dst) in enumerate(local)]
    for o in local:
        o.start()
    for o in local[:9]:
        o.wait()

    tab = (cr_ref[...], sr_ref[...], cc_ref[...], sc_ref[...])
    latent = root_scale(sl_ref[...], lg_ref[...]).astype(BF16)
    turned = turn(rk_ref[...].astype(F32), tab)
    for q in range(NY):
        kvbuf[z, c, q, 0:64, :] = latent[q * 64 : (q + 1) * 64]
        kvbuf[z, c, q, 64:80, :] = jnp.concatenate([turned[q * 8 : (q + 1) * 8], jnp.zeros((8, ROWS), F32)], axis=0).astype(BF16)
    qn = root_scale(ql_ref[...], qg_ref[...]).astype(BF16)
    narrow = dot(wqn_ref[...], qn, ((1,), (1,)))
    wide = dot(wqw_ref[...], qn, ((1,), (1,)))
    qbuf[x, 0:96, :] = jnp.concatenate([narrow[0:NOPE_A], turn(narrow[NOPE_A:], tab)], axis=0).astype(BF16)
    qbuf[x, 224:384, :] = jnp.concatenate([turn(wide[NOPE_B:], tab), wide[0:NOPE_B]], axis=0).astype(BF16)
    for j in range(NX):
        qbuf[j, 96:224, :] = jnp.zeros((128, ROWS), BF16)
    wk[:, 0:64] = kn_ref[...].T
    wk[:, 64:128] = jnp.zeros((LAT, 64), BF16)
    wk[:, 128:256] = kw_ref[...]
    wv[0:V_A, :] = vn_ref[...]
    wv[V_A:VD, :] = vw_ref[...].T

    pl.semaphore_wait(barrier, len(friends))

    for off in (1, 7, 2, 6, 3, 5, 4):
        send(kvbuf.at[z, c, t], kvbuf.at[z, c, t], M["KZ"] + off, dev_z(off))
    send(kvbuf.at[z, c], kvbuf.at[z, c], M["KT"], partner)
    for j in (2, 1, 3):
        for half, rows in enumerate((slice(0, 96), slice(224, 384))):
            send(qbuf.at[x, rows, :], qbuf.at[x, rows, :], M["Q"] + (j - 1) * 2 + half, dev_x(j))
    for o in local[9:12]:
        o.wait()

    def to_partner(u, zi, way):
        xi = at_x((0, -1, 1, 2)[way])
        send(b_slot(zi, xi), b_slot(zi, xi), M["PB"] + 4 * u + way, partner)

    def row_to_partner(u, zi):
        send(a_row(zi), a_row(zi), M["PA"] + u, partner)

    def to_x(u, zi):
        send(b_slot(zi, x), b_slot(zi, x), M["XP"] + u, dev_x(1))
        send(b_slot(zi, x), b_slot(zi, x), M["XM"] + u, dev_x(-1))

    def start_a():
        for j in (2, 1, 3):
            send(a_slot(z, x), a_slot(z, x), M["A1"] + j, dev_x(j))

    def start_b():
        send(b_slot(z, x), b_slot(z, x), M["BM"] + 1, dev_z(-1))
        send(b_slot(z, x), b_slot(z, x), M["BP"] + 1, dev_z(1))
        to_x(0, z)
        to_partner(0, z, 0)

    def start_rows():
        for j in range(1, NX):
            arrived(a_slot(z, at_x(-j)), M["A1"] + j)
        send(a_row(z), a_row(z), M["AM"] + 1, dev_z(-1))
        send(a_row(z), a_row(z), M["AP"] + 1, dev_z(1))
        row_to_partner(0, z)

    def rows_round(d):
        below, above = at_z(-d), at_z(d)
        cut = (lambda ref, half: ref) if d < 3 else lambda ref, half: ref.at[slice(2 * half, 2 * half + 2)]
        if d == 4:
            arrived(cut(a_row(below), 0), M["AP"] + d)
            arrived(cut(a_row(below), 1), M["AM"] + d)
            row_to_partner(7, below)
            return
        arrived(a_row(below), M["AP"] + d)
        send(cut(a_row(below), 0), cut(a_row(below), 0), M["AP"] + d + 1, dev_z(1))
        row_to_partner(2 * d - 1, below)
        arrived(a_row(above), M["AM"] + d)
        send(cut(a_row(above), 1), cut(a_row(above), 1), M["AM"] + d + 1, dev_z(-1))
        row_to_partner(2 * d, above)

    def slots_round(d, sideways=True):
        up, low = 2 * d - d // 4, 2 * d - 1
        arrived(b_slot(at_z(d), x), M["BM"] + d)
        if d < 4:
            send(b_slot(at_z(d), x), b_slot(at_z(d), x), M["BM"] + d + 1, dev_z(-1))
        to_partner(up, at_z(d), 0)
        if sideways:
            to_x(up, at_z(d))
        if d < 4:
            arrived(b_slot(at_z(-d), x), M["BP"] + d)
            if d < 3:
                send(b_slot(at_z(-d), x), b_slot(at_z(-d), x), M["BP"] + d + 1, dev_z(1))
            to_partner(low, at_z(-d), 0)
            if sideways:
                to_x(low, at_z(-d))

    plus = (0, 1, 3, 5)

    def relay(u):
        zu = zz(u)
        arrived(b_slot(zu, at_x(-1)), M["XP"] + u)
        if u in plus:
            send(b_slot(zu, at_x(-1)), b_slot(zu, at_x(-1)), M["RL"] + u, dev_x(1))
        to_partner(u, zu, 1)
        arrived(b_slot(zu, at_x(1)), M["XM"] + u)
        if u not in plus:
            send(b_slot(zu, at_x(1)), b_slot(zu, at_x(1)), M["RL"] + u, dev_x(-1))
        to_partner(u, zu, 2)

    def across(u):
        arrived(b_slot(zz(u), at_x(2)), M["RL"] + u)
        to_partner(u, zz(u), 3)

    def partner_block(u):
        for way in range(4):
            arrived(wbuf.at[zz(u), at_x((0, -1, 1, 2)[way]), 1 - c, :, B_COLS], M["PB"] + 4 * u + way)

    start_a()
    start_b()
    def send_wo():
        for j in (2, 1, 3):
            cols = pl.ds(pl.multiple_of(at_y(j) * DW, DW), DW)
            send(on_ref.at[:, cols], wo.at[t, 0:V_A, :], M["WO"] + (j - 1) * 2, dev_y(j))
            send(ow_ref.at[:, cols], wo.at[t, V_A:VD, :], M["WO"] + (j - 1) * 2 + 1, dev_y(j))

    for j in range(NX):
        ml[j] = jnp.concatenate([jnp.full((2, ROWS), -jnp.inf, F32), jnp.zeros((6, ROWS), F32)], axis=0)
        acc[j] = jnp.zeros((VD, ROWS), F32)

    def keys_of(zs):
        lane = lax.broadcasted_iota(jnp.int32, (ROWS, 128), 1)
        for core in range(2):
            latent = kvbuf[zs, core, :, 0:64, :].reshape(ROWS, LAT)
            turned = jnp.concatenate([kvbuf[zs, core, q, 64:80, :].astype(F32)[0:8] for q in range(NY)], axis=0)
            rot = jnp.concatenate([jnp.zeros((64, ROWS), F32), turned, turned], axis=0).T
            keys = dot(latent, wk[...], ((1,), (0,)))
            at = slice(core * ROWS, (core + 1) * ROWS)
            kx[at, 0:128] = jnp.where(lane < 64, keys[:, 0:128], rot).astype(BF16)
            kx[at, 128:256] = rot.astype(BF16)
            kx[at, 256:384] = keys[:, 128:256].astype(BF16)
            vx[:, at] = dot(wv[...], latent, ((1,), (1,))).astype(BF16)

    def attend(zs):
        keys_of(zs)

        heads = ((0, 128, 0, V_A, C_A), (128, 384, V_A, VD, C_B))
        every_score = [
            [dot(kx[:, lo:hi], qbuf[j, lo:hi, :], ((1,), (0,))) for lo, hi, _, _, _ in heads] for j in range(NX)
        ]
        for j in range(NX):
            for h, (_, _, vlo, vhi, scale) in enumerate(heads):
                scores = every_score[j][h]
                old = ml[j, h : h + 1, :]
                new = jnp.maximum(old, jnp.max(scores, axis=0, keepdims=True))
                factor = jnp.exp2((old - new) * scale)
                raised = jnp.exp2((scores - new) * scale)
                ml[j, h : h + 1, :] = new
                ml[j, 2 + h : 3 + h, :] = ml[j, 2 + h : 3 + h, :] * factor + jnp.sum(raised, axis=0, keepdims=True)
                acc[j, vlo:vhi, :] = acc[j, vlo:vhi, :] * factor + dot(vx[vlo:vhi, :], raised.astype(BF16), ((1,), (0,)))

    def quarter_out(u):
        d = (u + 1) // 2
        slot = kvbuf.at[zz(u), c, t]
        arrived(slot, M["KZ"] + (d if u % 2 else NZ - d))
        for j in (2, 1, 3):
            send(slot, slot, M["KY"] + 3 * u + j - 1, dev_y(j))

    def latents_across(u):
        zu = zz(u)
        for j in range(1, NY):
            arrived(kvbuf.at[zu, c, at_y(-j)], M["KY"] + 3 * u + j - 1)
        send(kvbuf.at[zu, c], kvbuf.at[zu, c], M["KT"] + u, partner)

    def on_step(k, value, then):
        @pl.when(k == value)
        def _():
            then()

    def unit(i, carry):
        @pl.when(i == 0)
        def _():
            quarter_out(1)
            quarter_out(2)
            for j in range(1, NX):
                for half, rows in enumerate((slice(0, 96), slice(224, 384))):
                    arrived(qbuf.at[at_x(-j), rows, :], M["Q"] + (j - 1) * 2 + half)
            quarter_out(3)
            quarter_out(4)

        on_step(i, 1, lambda: (quarter_out(5), quarter_out(6), quarter_out(7), send_wo(), slots_round(1)))
        on_step(i, 2, lambda: start_rows())
        on_step(i, 4, lambda: slots_round(2))

        @pl.when(i < 7)
        def _():
            latents_across(i + 1)

        zi = zz(i)
        arrived(kvbuf.at[zi, 1 - c], M["KT"] + i)
        attend(zi)
        return carry

    lax.fori_loop(0, NZ, unit, 0)

    for j in range(NX):
        for h, (vlo, vhi) in enumerate(((0, V_A), (V_A, VD))):
            osend[j, vlo:vhi, :] = (acc[j, vlo:vhi, :] / ml[j, 2 + h : 3 + h, :]).astype(BF16)
    for j in (2, 1, 3):
        send(osend.at[at_x(j)], orecv.at[j - 1], M["O"] + j, dev_x(j))
        send(ml.at[at_x(j)], srecv.at[j - 1], M["OS"] + j, dev_x(j))

    rows_round(1)
    slots_round(3)
    relay(0)
    for j in range(1, NX):
        arrived(orecv.at[j - 1], M["O"] + j)
        arrived(srecv.at[j - 1], M["OS"] + j)
    for h, (vlo, vhi, scale) in enumerate(((0, V_A, C_A), (V_A, VD, C_B))):
        tops = [ml[x, h : h + 1, :]] + [srecv[j, h : h + 1, :] for j in range(3)]
        sums = [ml[x, 2 + h : 3 + h, :]] + [srecv[j, 2 + h : 3 + h, :] for j in range(3)]
        parts = [osend[x, vlo:vhi, :]] + [orecv[j, vlo:vhi, :] for j in range(3)]
        top = jnp.maximum(jnp.maximum(tops[0], tops[1]), jnp.maximum(tops[2], tops[3]))
        shares = [total * jnp.exp2((m - top) * scale) for m, total in zip(tops, sums)]
        total = shares[0] + shares[1] + shares[2] + shares[3]
        mixed = sum(part.astype(F32) * (share / total) for part, share in zip(parts, shares))
        att[t, vlo:vhi, :] = mixed.astype(BF16)
    for j in (2, 1, 3):
        send(att.at[t], att.at[t], M["AT"] + j, dev_y(j))

    relay(1)
    relay(2)

    for o in local[12:]:
        o.wait()
    for j in range(1, NY):
        for half, rows in enumerate((slice(0, V_A), slice(V_A, VD))):
            arrived(wo.at[at_y(-j), rows, :], M["WO"] + (j - 1) * 2 + half)
    for j in range(1, NY):
        arrived(att.at[at_y(-j)], M["AT"] + j)

    def norm(stat, got, first, gain_ref, bias_ref, between):
        h = hres[...]
        center = jnp.mean(h, axis=1, keepdims=True)
        apart = jnp.sum((h - center) * (h - center), axis=1, keepdims=True)
        lane = lax.broadcasted_iota(jnp.int32, (ROWS, 128), 1)
        both = jnp.where(lane == 0, center, jnp.where(lane == 1, apart, 0.0))
        stat[...] = both.T[0:8]
        for j in (2, 1, 3):
            send(stat, got.at[j - 1], first + j, dev_y(j))
        between()
        for j in range(1, NY):
            arrived(got.at[j - 1], first + j)
        centers = [stat[0:1, :]] + [got[j, 0:1, :] for j in range(3)]
        aparts = [stat[1:2, :]] + [got[j, 1:2, :] for j in range(3)]
        middle = (centers[0] + centers[1] + centers[2] + centers[3]) * 0.25
        spread = sum(aparts) + DW * sum((m - middle) * (m - middle) for m in centers)
        root = lax.rsqrt(spread * (1.0 / D) + EPS_LAYER)
        cols = jnp.concatenate([middle, root, jnp.zeros((126, ROWS), F32)], axis=0).T
        return ((h - cols[:, 0:1]) * cols[:, 1:2] * gain_ref[...] + bias_ref[...]).astype(BF16)

    mixed = dot(att[...].reshape(NY * VD, ROWS), wo[...].reshape(NY * VD, DW), ((0,), (0,)))
    hres[...] = DEEP_ALPHA * res_ref[...].astype(F32) + mixed
    normed = norm(st1, sr1, M["S1"], g1_ref, b1_ref, lambda: (slots_round(4), relay(3)))
    xbuf[:, my_cols] = normed
    hres[...] = DEEP_ALPHA * normed.astype(F32)

    def x_half(off, half):
        return xbuf.at[pl.ds(half * HALF, HALF), pl.ds(pl.multiple_of(at_y(off) * DW, DW), DW)]

    def send_x(off, half, i, way):
        send(x_half(off, half), x_half(off, half), M["G"] + i, dev_y(way))

    for i, half, way in ((0, 0, 1), (2, 1, -1), (1, 1, 1), (3, 0, -1)):
        send_x(0, half, i, way)
    rows_round(2)
    relay(4)
    across(0)
    across(1)
    arrived(x_half(-1, 0), M["G"])
    send_x(-1, 0, 4, 1)
    arrived(x_half(1, 1), M["G"] + 2)
    send_x(1, 1, 5, -1)
    rows_round(3)
    relay(5)
    across(2)
    relay(6)
    across(3)
    relay(7)
    for i, off, half in ((1, -1, 1), (3, 1, 0), (4, 2, 0), (5, 2, 1)):
        arrived(x_half(off, half), M["G"] + i)

    def gate_up(u):
        zu = zz(u)
        features = xbuf[:, pl.ds(pl.multiple_of(zu * 256, 256), 256)]
        for n in range(WB // 256):
            cols = slice(n * 256, (n + 1) * 256)
            part = dot(features, wbuf[zu, :, :, :, cols].reshape(256, 256), ((1,), (0,)))
            gbuf[:, cols] = part if isinstance(u, int) else gbuf[:, cols] + part

    partner_block(0)
    gate_up(0)

    def block(u, carry):
        @pl.when(u <= 4)
        def _():
            across(u + 3)

        partner_block(u)
        gate_up(u)
        return carry

    lax.fori_loop(1, NZ, block, 0)
    rows_round(4)
    for u in range(NZ):
        arrived(wbuf.at[zz(u), :, 1 - c, :, A_COLS], M["PA"] + u)
    gbuf[:, WB:GU] = dot(xbuf[...], wbuf[:, :, :, :, WB:GU].reshape(D, 256), ((1,), (0,)))
    gate = gbuf[:, 0:FH]
    hid[...] = (gate / (1.0 + jnp.exp(-gate)) * gbuf[:, FH:GU]).astype(BF16)

    def feed(off):
        return dot(hid[...], wbuf[pl.ds(at_y(off) * 2, 2), :, :, :, GU:WT].reshape(DW, FH), ((1,), (1,)))

    first, second = slice(0, HALF), slice(HALF, ROWS)
    fsend[1] = feed(2).astype(BF16)
    send(fsend.at[1, first], fthru.at[0], M["F"], dev_y(1))
    send(fsend.at[1, second], fthru.at[1], M["F"] + 1, dev_y(-1))
    after = feed(1)
    fsend[0, second] = after[second].astype(BF16)
    send(fsend.at[0, second], frecv.at[0, second], M["F"] + 2, dev_y(1))
    fkeep[0] = after[first]
    before = feed(3)
    fsend[2, first] = before[first].astype(BF16)
    send(fsend.at[2, first], frecv.at[1, first], M["F"] + 3, dev_y(-1))
    fkeep[1] = before[second]
    arrived(fthru.at[0], M["F"])
    fsend[0, first] = (fkeep[0] + fthru[0].astype(F32)).astype(BF16)
    send(fsend.at[0, first], frecv.at[0, first], M["F"] + 4, dev_y(1))
    arrived(fthru.at[1], M["F"] + 1)
    fsend[2, second] = (fkeep[1] + fthru[1].astype(F32)).astype(BF16)
    send(fsend.at[2, second], frecv.at[1, second], M["F"] + 5, dev_y(-1))
    hres[...] += feed(0)
    for i, k, rows in ((2, 0, second), (3, 1, first), (4, 0, first), (5, 1, second)):
        arrived(frecv.at[k, rows], M["F"] + i)
    hres[...] += frecv[0].astype(F32) + frecv[1].astype(F32)
    out_ref[...] = norm(st2, sr2, M["S2"], g2_ref, b2_ref, lambda: None)

    for j in range(1, NX):
        sent(qbuf.at[0, 0:96, :], M["Q"] + (j - 1) * 2)
        sent(qbuf.at[0, 224:384, :], M["Q"] + (j - 1) * 2 + 1)
        sent(a_slot(0, 0), M["A1"] + j)
        sent(osend.at[0], M["O"] + j)
        sent(ml.at[0], M["OS"] + j)
        sent(wo.at[0, 0:V_A, :], M["WO"] + (j - 1) * 2)
        sent(wo.at[0, V_A:VD, :], M["WO"] + (j - 1) * 2 + 1)
        sent(att.at[0], M["AT"] + j)
        sent(st1, M["S1"] + j)
        sent(st2, M["S2"] + j)
    for d in range(1, 5):
        for way in "MP":
            sent(a_row(0) if d < 4 else a_row(0).at[0:2], M["A" + way] + d)
            if d < 4 or way == "M":
                sent(b_slot(0, 0), M["B" + way] + d)
    for u in range(NZ):
        sent(kvbuf.at[0, 0], M["KT"] + u)
        if u > 0:
            sent(kvbuf.at[0, 0, 0], M["KZ"] + u)
            for j in range(1, NY):
                sent(kvbuf.at[0, 0, 0], M["KY"] + 3 * u + j - 1)
        sent(a_row(0), M["PA"] + u)
        for way in range(4):
            sent(b_slot(0, 0), M["PB"] + 4 * u + way)
        for name in ("XP", "XM", "RL"):
            sent(b_slot(0, 0), M[name] + u)
    for i in range(6):
        sent(x_half(0, 0), M["G"] + i)
        sent(fsend.at[0, 0:HALF], M["F"] + i)


def body(
    residual, query_latent, shared_latent, rotary_key, query_gain, latent_gain, query_narrow, key_narrow,
    value_narrow, query_wide, key_wide, value_wide, output_narrow, output_wide, first_gain, first_bias,
    gate_weight, up_weight, down_weight, second_gain, second_bias,
):
    positions = lax.axis_index("sp") * ROWS + jnp.arange(ROWS, dtype=jnp.int32)
    quarter = ROPE // 4
    freqs = THETA ** (-(2.0 * jnp.arange(quarter, dtype=F32)) / (2 * quarter))
    row_angle = freqs[:, None] * (positions // GRID_W).astype(F32)[None, :]
    col_angle = freqs[:, None] * (positions % GRID_W).astype(F32)[None, :]
    row = lambda v: v.reshape(1, -1)
    large = (
        residual, query_latent, shared_latent, rotary_key.T, query_narrow.T, key_narrow.T, value_narrow.T,
        query_wide.T, key_wide, value_wide, output_narrow, output_wide, gate_weight, up_weight, down_weight.T,
    )
    small = (
        row(query_gain), row(latent_gain), row(first_gain), row(first_bias), row(second_gain), row(second_bias),
        jnp.cos(row_angle), jnp.sin(row_angle), jnp.cos(col_angle), jnp.sin(col_angle),
    )
    vmem = pl.BlockSpec(memory_space=pltpu.VMEM)
    return pl.pallas_call(
        layer_kernel,
        out_shape=jax.ShapeDtypeStruct((ROWS, DW), BF16),
        in_specs=[pl.BlockSpec(memory_space=pl.ANY)] * len(large) + [vmem] * len(small),
        out_specs=vmem,
        scratch_shapes=[
            *[pltpu.VMEM(v.shape, v.dtype) for v in large[:10]],
            pltpu.VMEM((NZ, 2, NY, 80, LAT), BF16),
            pltpu.VMEM((NX, KX, ROWS), BF16),
            pltpu.VMEM((NZ, NX, 2, SLOT, WT), BF16),
            pltpu.VMEM((LAT, 256), BF16),
            pltpu.VMEM((VD, LAT), BF16),
            pltpu.VMEM((2 * ROWS, KX), BF16),
            pltpu.VMEM((VD, 2 * ROWS), BF16),
            pltpu.VMEM((NX, 8, ROWS), F32),
            pltpu.VMEM((NX, VD, ROWS), F32),
            pltpu.VMEM((NX, VD, ROWS), BF16),
            pltpu.VMEM((3, VD, ROWS), BF16),
            pltpu.VMEM((3, 8, ROWS), F32),
            pltpu.VMEM((NY, VD, ROWS), BF16),
            pltpu.VMEM((NY, VD, DW), BF16),
            pltpu.VMEM((8, ROWS), F32),
            pltpu.VMEM((3, 8, ROWS), F32),
            pltpu.VMEM((8, ROWS), F32),
            pltpu.VMEM((3, 8, ROWS), F32),
            pltpu.VMEM((ROWS, D), BF16),
            pltpu.VMEM((ROWS, GU), F32),
            pltpu.VMEM((ROWS, FH), BF16),
            pltpu.VMEM((3, ROWS, DW), BF16),
            pltpu.VMEM((2, ROWS, DW), BF16),
            pltpu.VMEM((2, HALF, DW), BF16),
            pltpu.VMEM((2, HALF, DW), F32),
            pltpu.VMEM((ROWS, DW), F32),
            pltpu.SemaphoreType.DMA((MESSAGES,)),
            pltpu.SemaphoreType.DMA((MESSAGES,)),
            pltpu.SemaphoreType.DMA((len(large),)),
        ],
        compiler_params=pltpu.CompilerParams(
            collective_id=0, has_side_effects=True, vmem_limit_bytes=60 * 1024 * 1024
        ),
    )(*large, *small)


def solution(mesh):
    return jax.shard_map(
        body,
        mesh=mesh,
        in_specs=(
            P("sp", "tp"),
            P("sp", None),
            P("sp", None),
            P("sp", None),
            P(),
            P(),
            P(None, "tp"),
            P(None, "tp"),
            P(None, "tp"),
            P(None, "tp"),
            P(None, "tp"),
            P(None, "tp"),
            P("tp", None),
            P("tp", None),
            P("tp"),
            P("tp"),
            P("sp", "tp"),
            P("sp", "tp"),
            P("tp", "sp"),
            P("tp"),
            P("tp"),
        ),
        out_specs=P("sp", "tp"),
        check_vma=False,
    )
```

```python
import jax
import jax.numpy as jnp
from jax import lax
from jax.experimental import pallas as pl
from jax.experimental.pallas import tpu as pltpu
from jax.sharding import PartitionSpec as P

ROPE = 32
NOPE_A = 64
V_A = 64
NOPE_B = 128
V_B = 128
GRID_W = 64
EPS_ROOT = 1e-06
EPS_LAYER = 1e-05
THETA = 10000.0
DEEP_ALPHA = 2.0**0.25
LOG2E = 1.4426950408889634

NZ, NX, NY = 8, 4, 4
ROWS = 256
HALF = ROWS // 2
QUART = ROWS // 4
LAT = 256
DW = 512
D = 2048
FH = 1408
GU = 2 * FH
WT = 3 * FH
WB = GU - 512
B_COLS, A_COLS = slice(0, WB), slice(WB, WT)
SLOT = 32
VD = V_A + V_B
KX = 128 + 256
C_A = (NOPE_A + ROPE) ** -0.5 * LOG2E
C_B = (NOPE_B + ROPE) ** -0.5 * LOG2E
MESH = pl.DeviceIdType.MESH
F32, BF16 = jnp.float32, jnp.bfloat16


def numbered(**counts):
    at, table = 0, {}
    for name, count in counts.items():
        table[name] = at
        at += count
    return table, at


M, MESSAGES = numbered(
    Q=6, KZ=8, KY=24, KT=8, O=4, OS=4, WO=6, WP=4, RS=4, GN=8, AT=4, G=6, F=6, S2=4,
    A1=4, AM=20, AP=20, BM=5, BP=4, XP=8, XM=8, RL=8, PB=32, PA=8,
)


def dot(a, b, dims):
    return lax.dot_general(a, b, (dims, ((), ())), preferred_element_type=F32)


def root_scale(latent, gain):
    x = latent.astype(F32)
    return x * lax.rsqrt(jnp.mean(x * x, axis=-1, keepdims=True) + EPS_ROOT) * gain


def turn(v, tab):
    cr, sr, cc, sc = tab
    a, b, c, d = v[0:8], v[8:16], v[16:24], v[24:32]
    return jnp.concatenate([a * cr - b * sr, b * cr + a * sr, c * cc - d * sc, d * cc + c * sc], axis=0)


def layer_kernel(
    res_hbm, ql_hbm, sl_hbm, rk_hbm, wqn_hbm, kn_hbm, vn_hbm, wqw_hbm, kw_hbm, vw_hbm, on_ref, ow_ref,
    gate_ref, up_ref, down_ref, qg_ref, lg_ref, g1_ref, b1_ref, g2_ref, b2_ref, cr_ref, sr_ref, cc_ref, sc_ref,
    out_ref,
    ql_ref, sl_ref, rk_ref, wqn_ref, kn_ref, vn_ref, wqw_ref, kw_ref, vw_ref,
    kvbuf, qbuf, wbuf, wk, wv, kx, vx, ml, acc, osend, orecv, srecv, attended, attsend, att, wo, resq, gfull, st2, sr2,
    xbuf, gbuf, hid, fsend, frecv, fthru, fkeep, hres, ss, rs, ls,
):
    s, t = lax.axis_index("sp"), lax.axis_index("tp")
    c = lax.rem(s, 2)
    x = lax.rem(lax.div(s, 2), NX)
    z = lax.div(s, 2 * NX)

    def at_z(off):
        return lax.rem(z + off + NZ, NZ)

    def at_x(off):
        return lax.rem(x + off + NX, NX)

    def at_y(off):
        return lax.rem(t + off + NY, NY)

    def dev_z(off):
        return (at_z(off) * (2 * NX) + x * 2 + c, t)

    def dev_x(off):
        return (z * (2 * NX) + at_x(off) * 2 + c, t)

    def dev_y(off):
        return (s, at_y(off))

    partner = (s + 1 - 2 * c, t)

    def zz(u):
        return at_z(lax.div(u + 1, 2) * (1 - 2 * lax.rem(u, 2)) if not isinstance(u, int) else (u + 1) // 2 * (1 - 2 * (u % 2)))


    def msg(src, dst, i, dev):
        return pltpu.make_async_remote_copy(
            src_ref=src, dst_ref=dst, send_sem=ss.at[i], recv_sem=rs.at[i],
            device_id=dev, device_id_type=MESH,
        )

    def send(src, dst, i, dev):
        msg(src, dst, i, dev).start()

    def arrived(dst, i):
        msg(dst, dst, i, partner).wait_recv()

    def sent(src, i):
        msg(src, src, i, partner).wait_send()

    b_slot = lambda zi, xi: wbuf.at[zi, xi, c, :, B_COLS]
    a_slot = lambda zi, xi: wbuf.at[zi, xi, c, :, A_COLS]
    a_row = lambda zi: wbuf.at[zi, :, c, :, A_COLS]

    barrier = pltpu.get_barrier_semaphore()
    friends = [*[dev_z(off) for off in range(1, NZ)], dev_x(1), dev_x(2), dev_x(3), partner, dev_y(1), dev_y(2), dev_y(3)]
    for f in friends:
        pl.semaphore_signal(barrier, inc=1, device_id=f, device_id_type=MESH)

    my_cols = pl.ds(pl.multiple_of(t * DW, DW), DW)
    local = [
        (sl_hbm, sl_ref), (rk_hbm, rk_ref), (ql_hbm, ql_ref), (wqn_hbm, wqn_ref), (wqw_hbm, wqw_ref),
        (kn_hbm, kn_ref), (kw_hbm, kw_ref), (vn_hbm, vn_ref), (vw_hbm, vw_ref),
        (gate_ref, wbuf.at[z, x, c, :, 0:FH]), (up_ref, wbuf.at[z, x, c, :, FH:GU]),
        (down_ref, wbuf.at[z, x, c, :, GU:WT]), (on_ref, wo.at[t, 0:V_A, :]), (ow_ref, wo.at[t, V_A:VD, :]),
        (res_hbm.at[pl.ds(pl.multiple_of(t * QUART, QUART), QUART), :], resq.at[:, my_cols]),
        (g1_ref, gfull.at[0, :, my_cols]), (b1_ref, gfull.at[1, :, my_cols]),
    ]
    local = [pltpu.make_async_copy(src, dst, ls.at[i]) for i, (src, dst) in enumerate(local)]
    for o in local:
        o.start()
    for o in local[:9]:
        o.wait()

    tab = (cr_ref[...], sr_ref[...], cc_ref[...], sc_ref[...])
    latent = root_scale(sl_ref[...], lg_ref[...]).astype(BF16)
    turned = turn(rk_ref[...].astype(F32), tab)
    for q in range(NY):
        kvbuf[z, c, q, 0:64, :] = latent[q * 64 : (q + 1) * 64]
        kvbuf[z, c, q, 64:80, :] = jnp.concatenate([turned[q * 8 : (q + 1) * 8], jnp.zeros((8, ROWS), F32)], axis=0).astype(BF16)
    qn = root_scale(ql_ref[...], qg_ref[...]).astype(BF16)
    narrow = dot(wqn_ref[...], qn, ((1,), (1,)))
    wide = dot(wqw_ref[...], qn, ((1,), (1,)))
    qbuf[x, 0:96, :] = jnp.concatenate([narrow[0:NOPE_A], turn(narrow[NOPE_A:], tab)], axis=0).astype(BF16)
    qbuf[x, 224:384, :] = jnp.concatenate([turn(wide[NOPE_B:], tab), wide[0:NOPE_B]], axis=0).astype(BF16)
    for j in range(NX):
        qbuf[j, 96:224, :] = jnp.zeros((128, ROWS), BF16)
    wk[:, 0:64] = kn_ref[...].T
    wk[:, 64:128] = jnp.zeros((LAT, 64), BF16)
    wk[:, 128:256] = kw_ref[...]
    wv[0:V_A, :] = vn_ref[...]
    wv[V_A:VD, :] = vw_ref[...].T

    pl.semaphore_wait(barrier, len(friends))

    for off in (1, 7, 2, 6, 3, 5, 4):
        send(kvbuf.at[z, c, t], kvbuf.at[z, c, t], M["KZ"] + off, dev_z(off))
    send(kvbuf.at[z, c], kvbuf.at[z, c], M["KT"], partner)
    for j in (2, 1, 3):
        for half, rows in enumerate((slice(0, 96), slice(224, 384))):
            send(qbuf.at[x, rows, :], qbuf.at[x, rows, :], M["Q"] + (j - 1) * 2 + half, dev_x(j))
    for o in local[9:12]:
        o.wait()

    def to_partner(u, zi, way):
        xi = at_x((0, -1, 1, 2)[way])
        send(b_slot(zi, xi), b_slot(zi, xi), M["PB"] + 4 * u + way, partner)

    def row_to_partner(u, zi):
        send(a_row(zi), a_row(zi), M["PA"] + u, partner)

    def to_x(u, zi):
        send(b_slot(zi, x), b_slot(zi, x), M["XP"] + u, dev_x(1))
        send(b_slot(zi, x), b_slot(zi, x), M["XM"] + u, dev_x(-1))

    def send_rows(zi, d, r):
        slot = a_slot(zi, at_x(-r))
        send(slot, slot, M["AP"] + 4 * d + r, dev_z(1))
        send(slot, slot, M["AM"] + 4 * d + r, dev_z(-1))

    def start_a():
        send_rows(z, 1, 0)
        for j in (2, 1, 3):
            send(a_slot(z, x), a_slot(z, x), M["A1"] + j, dev_x(j))

    def start_b():
        send(b_slot(z, x), b_slot(z, x), M["BM"] + 1, dev_z(-1))
        send(b_slot(z, x), b_slot(z, x), M["BP"] + 1, dev_z(1))
        to_partner(0, z, 0)

    def start_rows():
        for r in (1, 3, 2):
            arrived(a_slot(z, at_x(-r)), M["A1"] + r)
            send_rows(z, 1, r)
        row_to_partner(0, z)

    def rows_round(d, *rs):
        below, above = at_z(-d), at_z(d)
        for r in rs:
            if d < 4 or r < 2:
                arrived(a_slot(below, at_x(-r)), M["AP"] + 4 * d + r)
            if d < 3 or d == 3 and r < 2:
                send(a_slot(below, at_x(-r)), a_slot(below, at_x(-r)), M["AP"] + 4 * d + 4 + r, dev_z(1))
            if d < 4 or r >= 2:
                arrived(a_slot(above, at_x(-r)), M["AM"] + 4 * d + r)
            if d < 3 or d == 3 and r >= 2:
                send(a_slot(above, at_x(-r)), a_slot(above, at_x(-r)), M["AM"] + 4 * d + 4 + r, dev_z(-1))
            if r == 2:
                row_to_partner(2 * d - 1, below)
                if d < 4:
                    row_to_partner(2 * d, above)

    def slots_round(d, sideways=True):
        up, low = 2 * d - d // 4, 2 * d - 1
        arrived(b_slot(at_z(d), x), M["BM"] + d)
        if d < 4:
            send(b_slot(at_z(d), x), b_slot(at_z(d), x), M["BM"] + d + 1, dev_z(-1))
        to_partner(up, at_z(d), 0)
        if sideways:
            to_x(up, at_z(d))
        if d < 4:
            arrived(b_slot(at_z(-d), x), M["BP"] + d)
            if d < 3:
                send(b_slot(at_z(-d), x), b_slot(at_z(-d), x), M["BP"] + d + 1, dev_z(1))
            to_partner(low, at_z(-d), 0)
            if sideways:
                to_x(low, at_z(-d))

    plus = (0, 1, 3, 5)

    def relay(u):
        zu = zz(u)
        arrived(b_slot(zu, at_x(-1)), M["XP"] + u)
        if u in plus:
            send(b_slot(zu, at_x(-1)), b_slot(zu, at_x(-1)), M["RL"] + u, dev_x(1))
        to_partner(u, zu, 1)
        arrived(b_slot(zu, at_x(1)), M["XM"] + u)
        if u not in plus:
            send(b_slot(zu, at_x(1)), b_slot(zu, at_x(1)), M["RL"] + u, dev_x(-1))
        to_partner(u, zu, 2)

    def across(u):
        arrived(b_slot(zz(u), at_x(2)), M["RL"] + u)
        to_partner(u, zz(u), 3)

    def partner_block(u):
        for way in range(4):
            arrived(wbuf.at[zz(u), at_x((0, -1, 1, 2)[way]), 1 - c, :, B_COLS], M["PB"] + 4 * u + way)

    start_b()
    start_a()
    to_x(0, z)
    wo_half = lambda core: pl.ds(pl.multiple_of(core * (D // 2), D // 2), D // 2)

    def send_wo():
        for j in (2, 1, 3):
            rows = pl.ds(pl.multiple_of(at_y(j) * QUART, QUART), QUART)
            send(res_hbm.at[rows, :], resq.at[:, my_cols], M["RS"] + j, dev_y(j))
            send(g1_ref, gfull.at[0, :, my_cols], M["GN"] + j, dev_y(j))
            send(b1_ref, gfull.at[1, :, my_cols], M["GN"] + 4 + j, dev_y(j))
        for j in (2, 1, 3):
            send(on_ref.at[:, wo_half(c)], wo.at[t, 0:V_A, wo_half(c)], M["WO"] + (j - 1) * 2, dev_y(j))
            send(ow_ref.at[:, wo_half(c)], wo.at[t, V_A:VD, wo_half(c)], M["WO"] + (j - 1) * 2 + 1, dev_y(j))

    def wo_across():
        for j in range(1, NY):
            arrived(wo.at[at_y(-j), 0:V_A, wo_half(c)], M["WO"] + (j - 1) * 2)
            arrived(wo.at[at_y(-j), V_A:VD, wo_half(c)], M["WO"] + (j - 1) * 2 + 1)
            send(wo.at[at_y(-j), :, wo_half(c)], wo.at[at_y(-j), :, wo_half(c)], M["WP"] + j, partner)

    for j in range(NX):
        ml[j] = jnp.concatenate([jnp.full((2, ROWS), -jnp.inf, F32), jnp.zeros((6, ROWS), F32)], axis=0)
        acc[j] = jnp.zeros((VD, ROWS), F32)

    def keys_of(zs):
        lane = lax.broadcasted_iota(jnp.int32, (ROWS, 128), 1)
        for core in range(2):
            latent = kvbuf[zs, core, :, 0:64, :].reshape(ROWS, LAT)
            turned = jnp.concatenate([kvbuf[zs, core, q, 64:80, :].astype(F32)[0:8] for q in range(NY)], axis=0)
            rot = jnp.concatenate([jnp.zeros((64, ROWS), F32), turned, turned], axis=0).T
            keys = dot(latent, wk[...], ((1,), (0,)))
            at = slice(core * ROWS, (core + 1) * ROWS)
            kx[at, 0:128] = jnp.where(lane < 64, keys[:, 0:128], rot).astype(BF16)
            kx[at, 128:256] = rot.astype(BF16)
            kx[at, 256:384] = keys[:, 128:256].astype(BF16)
            vx[:, at] = dot(wv[...], latent, ((1,), (1,))).astype(BF16)

    def attend(zs):
        keys_of(zs)

        heads = ((0, 128, 0, V_A, C_A), (128, 384, V_A, VD, C_B))
        every_score = [
            [dot(kx[:, lo:hi], qbuf[j, lo:hi, :], ((1,), (0,))) for lo, hi, _, _, _ in heads] for j in range(NX)
        ]
        for j in range(NX):
            for h, (_, _, vlo, vhi, scale) in enumerate(heads):
                scores = every_score[j][h]
                old = ml[j, h : h + 1, :]
                new = jnp.maximum(old, jnp.max(scores, axis=0, keepdims=True))
                factor = jnp.exp2((old - new) * scale)
                raised = jnp.exp2((scores - new) * scale).astype(BF16)
                ml[j, h : h + 1, :] = new
                with_ones = jnp.concatenate([vx[vlo:vhi, :], jnp.ones((16, 2 * ROWS), BF16)], axis=0)
                product = dot(with_ones, raised, ((1,), (0,)))
                ml[j, 2 + h : 3 + h, :] = ml[j, 2 + h : 3 + h, :] * factor + product[vhi - vlo : vhi - vlo + 1]
                acc[j, vlo:vhi, :] = acc[j, vlo:vhi, :] * factor + product[0 : vhi - vlo]

    def quarter_out(u):
        d = (u + 1) // 2
        slot = kvbuf.at[zz(u), c, t]
        arrived(slot, M["KZ"] + (d if u % 2 else NZ - d))
        for j in (2, 1, 3):
            send(slot, slot, M["KY"] + 3 * u + j - 1, dev_y(j))

    def latents_across(u):
        zu = zz(u)
        for j in range(1, NY):
            arrived(kvbuf.at[zu, c, at_y(-j)], M["KY"] + 3 * u + j - 1)
        send(kvbuf.at[zu, c], kvbuf.at[zu, c], M["KT"] + u, partner)

    def on_step(k, value, then):
        @pl.when(k == value)
        def _():
            then()

    def unit(i, carry):
        @pl.when(i == 0)
        def _():
            quarter_out(1)
            quarter_out(2)
            for j in range(1, NX):
                for half, rows in enumerate((slice(0, 96), slice(224, 384))):
                    arrived(qbuf.at[at_x(-j), rows, :], M["Q"] + (j - 1) * 2 + half)
            quarter_out(3)
            quarter_out(4)

        on_step(i, 1, lambda: (quarter_out(5), quarter_out(6), quarter_out(7), send_wo(), slots_round(1)))
        on_step(i, 2, lambda: start_rows())
        on_step(i, 3, lambda: rows_round(1, 0))
        on_step(i, 4, lambda: slots_round(2))
        on_step(i, 6, lambda: rows_round(1, 1, 3))

        @pl.when(i < 7)
        def _():
            latents_across(i + 1)

        zi = zz(i)
        arrived(kvbuf.at[zi, 1 - c], M["KT"] + i)
        attend(zi)
        return carry

    lax.fori_loop(0, NZ, unit, 0)

    for j in range(NX):
        for h, (vlo, vhi) in enumerate(((0, V_A), (V_A, VD))):
            osend[j, vlo:vhi, :] = (acc[j, vlo:vhi, :] / ml[j, 2 + h : 3 + h, :]).astype(BF16)
    for j in (2, 1, 3):
        send(osend.at[at_x(j)], orecv.at[j - 1], M["O"] + j, dev_x(j))
        send(ml.at[at_x(j)], srecv.at[j - 1], M["OS"] + j, dev_x(j))

    rows_round(1, 2)
    rows_round(2, 0)
    slots_round(3)
    relay(0)
    for j in range(1, NX):
        arrived(orecv.at[j - 1], M["O"] + j)
        arrived(srecv.at[j - 1], M["OS"] + j)
    for h, (vlo, vhi, scale) in enumerate(((0, V_A, C_A), (V_A, VD, C_B))):
        tops = [ml[x, h : h + 1, :]] + [srecv[j, h : h + 1, :] for j in range(3)]
        sums = [ml[x, 2 + h : 3 + h, :]] + [srecv[j, 2 + h : 3 + h, :] for j in range(3)]
        parts = [osend[x, vlo:vhi, :]] + [orecv[j, vlo:vhi, :] for j in range(3)]
        top = jnp.maximum(jnp.maximum(tops[0], tops[1]), jnp.maximum(tops[2], tops[3]))
        shares = [total * jnp.exp2((m - top) * scale) for m, total in zip(tops, sums)]
        total = shares[0] + shares[1] + shares[2] + shares[3]
        mixed = sum(part.astype(F32) * (share / total) for part, share in zip(parts, shares))
        attended[vlo:vhi, :] = mixed
    mine = attended[...].T.astype(BF16)
    for q in range(NY):
        attsend[q] = mine[q * QUART : (q + 1) * QUART]
    for j in (2, 1, 3):
        send(attsend.at[at_y(j)], att.at[t], M["AT"] + j, dev_y(j))

    wo_across()
    rows_round(2, 1)
    relay(1)
    rows_round(2, 3)
    relay(2)

    for o in local[12:]:
        o.wait()
    for j in range(1, NY):
        arrived(resq.at[:, pl.ds(pl.multiple_of(at_y(-j) * DW, DW), DW)], M["RS"] + j)
        arrived(gfull.at[0, :, pl.ds(pl.multiple_of(at_y(-j) * DW, DW), DW)], M["GN"] + j)
        arrived(gfull.at[1, :, pl.ds(pl.multiple_of(at_y(-j) * DW, DW), DW)], M["GN"] + 4 + j)
        arrived(wo.at[at_y(-j), :, wo_half(1 - c)], M["WP"] + j)
    for j in range(1, NY):
        arrived(att.at[at_y(-j)], M["AT"] + j)

    def norm(stat, got, first, gain_ref, bias_ref):
        h = hres[...]
        center = jnp.mean(h, axis=1, keepdims=True)
        apart = jnp.sum((h - center) * (h - center), axis=1, keepdims=True)
        lane = lax.broadcasted_iota(jnp.int32, (ROWS, 128), 1)
        both = jnp.where(lane == 0, center, jnp.where(lane == 1, apart, 0.0))
        stat[...] = both.T[0:8]
        for j in (2, 1, 3):
            send(stat, got.at[j - 1], first + j, dev_y(j))
        for j in range(1, NY):
            arrived(got.at[j - 1], first + j)
        centers = [stat[0:1, :]] + [got[j, 0:1, :] for j in range(3)]
        aparts = [stat[1:2, :]] + [got[j, 1:2, :] for j in range(3)]
        middle = (centers[0] + centers[1] + centers[2] + centers[3]) * 0.25
        spread = sum(aparts) + DW * sum((m - middle) * (m - middle) for m in centers)
        root = lax.rsqrt(spread * (1.0 / D) + EPS_LAYER)
        cols = jnp.concatenate([middle, root, jnp.zeros((126, ROWS), F32)], axis=0).T
        return ((h - cols[:, 0:1]) * cols[:, 1:2] * gain_ref[...] + bias_ref[...]).astype(BF16)

    h = DEEP_ALPHA * resq[...].astype(F32) + dot(attsend[t], wo[t], ((1,), (0,)))
    for j in range(1, NY):
        h = h + dot(att[at_y(j)], wo[at_y(j)], ((1,), (0,)))
    center = jnp.mean(h, axis=1, keepdims=True)
    spread = jnp.mean((h - center) * (h - center), axis=1, keepdims=True)
    my_rows = pl.ds(pl.multiple_of(t * QUART, QUART), QUART)
    xbuf[my_rows, :] = ((h - center) * lax.rsqrt(spread + EPS_LAYER) * gfull[0] + gfull[1]).astype(BF16)

    def x_half(off, half):
        return xbuf.at[pl.ds(pl.multiple_of(at_y(off) * QUART, QUART), QUART), pl.ds(half * (D // 2), D // 2)]

    def send_x(off, half, i, way):
        send(x_half(off, half), x_half(off, half), M["G"] + i, dev_y(way))

    for i, half, way in ((0, 0, 1), (2, 1, -1), (1, 1, 1), (3, 0, -1)):
        send_x(0, half, i, way)
    slots_round(4)
    rows_round(2, 2)
    relay(3)
    rows_round(3, 0)
    relay(4)
    across(0)
    across(1)
    arrived(x_half(-1, 0), M["G"])
    send_x(-1, 0, 4, 1)
    arrived(x_half(1, 1), M["G"] + 2)
    send_x(1, 1, 5, -1)
    rows_round(3, 1)
    relay(5)
    across(2)
    rows_round(3, 3)
    relay(6)
    across(3)
    rows_round(3, 2)
    relay(7)
    for i, off, half in ((1, -1, 1), (3, 1, 0), (4, 2, 0), (5, 2, 1)):
        arrived(x_half(off, half), M["G"] + i)

    hres[...] = DEEP_ALPHA * xbuf[:, my_cols].astype(F32)

    def gate_up(u):
        zu = zz(u)
        features = xbuf[:, pl.ds(pl.multiple_of(zu * 256, 256), 256)]
        for n in range(GU // 256):
            cols = slice(n * 256, (n + 1) * 256)
            part = dot(features, wbuf[zu, :, :, :, cols].reshape(256, 256), ((1,), (0,)))
            gbuf[:, cols] = part if isinstance(u, int) else gbuf[:, cols] + part

    def partner_rows(u):
        arrived(wbuf.at[zz(u), :, 1 - c, :, A_COLS], M["PA"] + u)

    partner_block(0)
    partner_rows(0)
    gate_up(0)

    def block(u, carry):
        @pl.when(u <= 4)
        def _():
            across(u + 3)

        on_step(u, 5, lambda: rows_round(4, 0, 1, 3, 2))

        partner_block(u)
        partner_rows(u)
        gate_up(u)
        return carry

    lax.fori_loop(1, NZ, block, 0)
    gate = gbuf[:, 0:FH]
    hid[...] = (gate / (1.0 + jnp.exp(-gate)) * gbuf[:, FH:GU]).astype(BF16)

    def feed(off):
        return dot(hid[...], wbuf[pl.ds(at_y(off) * 2, 2), :, :, :, GU:WT].reshape(DW, FH), ((1,), (1,)))

    first, second = slice(0, HALF), slice(HALF, ROWS)
    fsend[1] = feed(2).astype(BF16)
    send(fsend.at[1, first], fthru.at[0], M["F"], dev_y(1))
    send(fsend.at[1, second], fthru.at[1], M["F"] + 1, dev_y(-1))
    after = feed(1)
    fsend[0, second] = after[second].astype(BF16)
    send(fsend.at[0, second], frecv.at[0, second], M["F"] + 2, dev_y(1))
    fkeep[0] = after[first]
    before = feed(3)
    fsend[2, first] = before[first].astype(BF16)
    send(fsend.at[2, first], frecv.at[1, first], M["F"] + 3, dev_y(-1))
    fkeep[1] = before[second]
    arrived(fthru.at[0], M["F"])
    fsend[0, first] = (fkeep[0] + fthru[0].astype(F32)).astype(BF16)
    send(fsend.at[0, first], frecv.at[0, first], M["F"] + 4, dev_y(1))
    arrived(fthru.at[1], M["F"] + 1)
    fsend[2, second] = (fkeep[1] + fthru[1].astype(F32)).astype(BF16)
    send(fsend.at[2, second], frecv.at[1, second], M["F"] + 5, dev_y(-1))
    hres[...] += feed(0)
    for i, k, rows in ((2, 0, second), (3, 1, first), (4, 0, first), (5, 1, second)):
        arrived(frecv.at[k, rows], M["F"] + i)
    hres[...] += frecv[0].astype(F32) + frecv[1].astype(F32)
    out_ref[...] = norm(st2, sr2, M["S2"], g2_ref, b2_ref)

    for j in range(1, NX):
        sent(qbuf.at[0, 0:96, :], M["Q"] + (j - 1) * 2)
        sent(qbuf.at[0, 224:384, :], M["Q"] + (j - 1) * 2 + 1)
        sent(a_slot(0, 0), M["A1"] + j)
        sent(osend.at[0], M["O"] + j)
        sent(ml.at[0], M["OS"] + j)
        sent(wo.at[0, 0:V_A, wo_half(0)], M["WO"] + (j - 1) * 2)
        sent(wo.at[0, V_A:VD, wo_half(0)], M["WO"] + (j - 1) * 2 + 1)
        sent(wo.at[0, :, wo_half(0)], M["WP"] + j)
        sent(resq.at[:, my_cols], M["RS"] + j)
        sent(g1_ref, M["GN"] + j)
        sent(b1_ref, M["GN"] + 4 + j)
        sent(att.at[0], M["AT"] + j)
        sent(st2, M["S2"] + j)
    for d in range(1, 5):
        for way in "MP":
            for r in range(4):
                if d < 4 or (r >= 2) == (way == "M"):
                    sent(a_slot(0, 0), M["A" + way] + 4 * d + r)
            if d < 4 or way == "M":
                sent(b_slot(0, 0), M["B" + way] + d)
    for u in range(NZ):
        sent(kvbuf.at[0, 0], M["KT"] + u)
        if u > 0:
            sent(kvbuf.at[0, 0, 0], M["KZ"] + u)
            for j in range(1, NY):
                sent(kvbuf.at[0, 0, 0], M["KY"] + 3 * u + j - 1)
        sent(a_row(0), M["PA"] + u)
        for way in range(4):
            sent(b_slot(0, 0), M["PB"] + 4 * u + way)
        for name in ("XP", "XM", "RL"):
            sent(b_slot(0, 0), M[name] + u)
    for i in range(6):
        sent(x_half(0, 0), M["G"] + i)
        sent(fsend.at[0, 0:HALF], M["F"] + i)


def body(
    residual, query_latent, shared_latent, rotary_key, query_gain, latent_gain, query_narrow, key_narrow,
    value_narrow, query_wide, key_wide, value_wide, output_narrow, output_wide, first_gain, first_bias,
    gate_weight, up_weight, down_weight, second_gain, second_bias,
):
    positions = lax.axis_index("sp") * ROWS + jnp.arange(ROWS, dtype=jnp.int32)
    quarter = ROPE // 4
    freqs = THETA ** (-(2.0 * jnp.arange(quarter, dtype=F32)) / (2 * quarter))
    row_angle = freqs[:, None] * (positions // GRID_W).astype(F32)[None, :]
    col_angle = freqs[:, None] * (positions % GRID_W).astype(F32)[None, :]
    row = lambda v: v.reshape(1, -1)
    large = (
        residual, query_latent, shared_latent, rotary_key.T, query_narrow.T, key_narrow.T, value_narrow.T,
        query_wide.T, key_wide, value_wide, output_narrow, output_wide, gate_weight, up_weight, down_weight.T,
    )
    small = (
        row(query_gain), row(latent_gain), row(first_gain), row(first_bias), row(second_gain), row(second_bias),
        jnp.cos(row_angle), jnp.sin(row_angle), jnp.cos(col_angle), jnp.sin(col_angle),
    )
    vmem = pl.BlockSpec(memory_space=pltpu.VMEM)
    return pl.pallas_call(
        layer_kernel,
        out_shape=jax.ShapeDtypeStruct((ROWS, DW), BF16),
        in_specs=[pl.BlockSpec(memory_space=pl.ANY)] * len(large) + [vmem] * len(small),
        out_specs=vmem,
        scratch_shapes=[
            *[pltpu.VMEM(v.shape, v.dtype) for v in large[1:10]],
            pltpu.VMEM((NZ, 2, NY, 80, LAT), BF16),
            pltpu.VMEM((NX, KX, ROWS), BF16),
            pltpu.VMEM((NZ, NX, 2, SLOT, WT), BF16),
            pltpu.VMEM((LAT, 256), BF16),
            pltpu.VMEM((VD, LAT), BF16),
            pltpu.VMEM((2 * ROWS, KX), BF16),
            pltpu.VMEM((VD, 2 * ROWS), BF16),
            pltpu.VMEM((NX, 8, ROWS), F32),
            pltpu.VMEM((NX, VD, ROWS), F32),
            pltpu.VMEM((NX, VD, ROWS), BF16),
            pltpu.VMEM((3, VD, ROWS), BF16),
            pltpu.VMEM((3, 8, ROWS), F32),
            pltpu.VMEM((VD, ROWS), F32),
            pltpu.VMEM((NY, QUART, VD), BF16),
            pltpu.VMEM((NY, QUART, VD), BF16),
            pltpu.VMEM((NY, VD, D), BF16),
            pltpu.VMEM((QUART, D), BF16),
            pltpu.VMEM((2, 1, D), F32),
            pltpu.VMEM((8, ROWS), F32),
            pltpu.VMEM((3, 8, ROWS), F32),
            pltpu.VMEM((ROWS, D), BF16),
            pltpu.VMEM((ROWS, GU), F32),
            pltpu.VMEM((ROWS, FH), BF16),
            pltpu.VMEM((3, ROWS, DW), BF16),
            pltpu.VMEM((2, ROWS, DW), BF16),
            pltpu.VMEM((2, HALF, DW), BF16),
            pltpu.VMEM((2, HALF, DW), F32),
            pltpu.VMEM((ROWS, DW), F32),
            pltpu.SemaphoreType.DMA((MESSAGES,)),
            pltpu.SemaphoreType.DMA((MESSAGES,)),
            pltpu.SemaphoreType.DMA((len(large) + 2,)),
        ],
        compiler_params=pltpu.CompilerParams(
            collective_id=0, has_side_effects=True, vmem_limit_bytes=60 * 1024 * 1024
        ),
    )(*large, *small)


def solution(mesh):
    return jax.shard_map(
        body,
        mesh=mesh,
        in_specs=(
            P("sp", "tp"),
            P("sp", None),
            P("sp", None),
            P("sp", None),
            P(),
            P(),
            P(None, "tp"),
            P(None, "tp"),
            P(None, "tp"),
            P(None, "tp"),
            P(None, "tp"),
            P(None, "tp"),
            P("tp", None),
            P("tp", None),
            P("tp"),
            P("tp"),
            P("sp", "tp"),
            P("sp", "tp"),
            P("tp", "sp"),
            P("tp"),
            P("tp"),
        ),
        out_specs=P("sp", "tp"),
        check_vma=False,
    )
```

```python
import jax
import jax.numpy as jnp
from jax import lax
from jax.experimental import pallas as pl
from jax.experimental.pallas import tpu as pltpu
from jax.sharding import PartitionSpec as P

ROPE = 32
NOPE_A = 64
V_A = 64
NOPE_B = 128
V_B = 128
GRID_W = 64
EPS_ROOT = 1e-06
EPS_LAYER = 1e-05
THETA = 10000.0
DEEP_ALPHA = 2.0**0.25
LOG2E = 1.4426950408889634

NZ, NX, NY = 8, 4, 4
ROWS = 256
HALF = ROWS // 2
QUART = ROWS // 4
LAT = 256
DW = 512
D = 2048
FH = 1408
GU = 2 * FH
WT = 3 * FH
WB = GU - 640
B_COLS, A_COLS = slice(0, WB), slice(WB, WT)
SLOT = 32
VD = V_A + V_B
KX = 128 + 256
C_A = (NOPE_A + ROPE) ** -0.5 * LOG2E
C_B = (NOPE_B + ROPE) ** -0.5 * LOG2E
MESH = pl.DeviceIdType.MESH
F32, BF16 = jnp.float32, jnp.bfloat16


def numbered(**counts):
    at, table = 0, {}
    for name, count in counts.items():
        table[name] = at
        at += count
    return table, at


M, MESSAGES = numbered(
    Q=6, KM=5, KP=4, KY=24, KT=8, O=4, OS=4, WO=6, WP=4, RS=4, GN=8, AT=4, G=6, F=6, S2=4,
    A1=4, AM=20, AP=20, BM=5, BP=4, XP=8, XM=8, RL=9, PB=32, PA=8,
)


def dot(a, b, dims):
    return lax.dot_general(a, b, (dims, ((), ())), preferred_element_type=F32)


def root_scale(latent, gain):
    x = latent.astype(F32)
    return x * lax.rsqrt(jnp.mean(x * x, axis=-1, keepdims=True) + EPS_ROOT) * gain


def turn(v, tab):
    cr, sr, cc, sc = tab
    a, b, c, d = v[0:8], v[8:16], v[16:24], v[24:32]
    return jnp.concatenate([a * cr - b * sr, b * cr + a * sr, c * cc - d * sc, d * cc + c * sc], axis=0)


def layer_kernel(
    res_hbm, ql_hbm, sl_hbm, rk_hbm, wqn_hbm, kn_hbm, vn_hbm, wqw_hbm, kw_hbm, vw_hbm, on_ref, ow_ref,
    gate_ref, up_ref, down_ref, qg_ref, lg_ref, g1_ref, b1_ref, g2_ref, b2_ref,
    out_ref,
    ql_ref, sl_ref, rk_ref, wqn_ref, kn_ref, vn_ref, wqw_ref, kw_ref, vw_ref,
    kvbuf, qbuf, wbuf, wk, wv, kx, vx, ml, acc, osend, orecv, srecv, attended, attsend, att, wo, resq, gfull, st2, sr2,
    xbuf, gbuf, hid, fsend, frecv, fthru, fkeep, hres, ss, rs, ls,
):
    s, t = lax.axis_index("sp"), lax.axis_index("tp")
    c = lax.rem(s, 2)
    x = lax.rem(lax.div(s, 2), NX)
    z = lax.div(s, 2 * NX)

    def at_z(off):
        return lax.rem(z + off + NZ, NZ)

    def at_x(off):
        return lax.rem(x + off + NX, NX)

    def at_y(off):
        return lax.rem(t + off + NY, NY)

    def dev_z(off):
        return (at_z(off) * (2 * NX) + x * 2 + c, t)

    def dev_x(off):
        return (z * (2 * NX) + at_x(off) * 2 + c, t)

    def dev_y(off):
        return (s, at_y(off))

    partner = (s + 1 - 2 * c, t)

    def zz(u):
        return at_z(lax.div(u + 1, 2) * (1 - 2 * lax.rem(u, 2)) if not isinstance(u, int) else (u + 1) // 2 * (1 - 2 * (u % 2)))


    def msg(src, dst, i, dev):
        return pltpu.make_async_remote_copy(
            src_ref=src, dst_ref=dst, send_sem=ss.at[i], recv_sem=rs.at[i],
            device_id=dev, device_id_type=MESH,
        )

    def send(src, dst, i, dev):
        msg(src, dst, i, dev).start()

    def arrived(dst, i):
        msg(dst, dst, i, partner).wait_recv()

    def sent(src, i):
        msg(src, src, i, partner).wait_send()

    b_slot = lambda zi, xi: wbuf.at[zi, xi, c, :, B_COLS]
    a_slot = lambda zi, xi: wbuf.at[zi, xi, c, :, A_COLS]
    a_row = lambda zi: wbuf.at[zi, :, c, :, A_COLS]

    barrier = pltpu.get_barrier_semaphore()
    friends = [dev_z(1), dev_z(-1), dev_x(1), dev_x(2), dev_x(3), partner, dev_y(1), dev_y(2), dev_y(3)]
    for f in friends:
        pl.semaphore_signal(barrier, inc=1, device_id=f, device_id_type=MESH)

    my_cols = pl.ds(pl.multiple_of(t * DW, DW), DW)
    local = [
        (sl_hbm, sl_ref), (rk_hbm, rk_ref), (ql_hbm, ql_ref), (wqn_hbm, wqn_ref), (wqw_hbm, wqw_ref),
        (kn_hbm, kn_ref), (kw_hbm, kw_ref), (vn_hbm, vn_ref), (vw_hbm, vw_ref),
        (gate_ref, wbuf.at[z, x, c, :, 0:FH]), (up_ref, wbuf.at[z, x, c, :, FH:GU]),
        (down_ref, wbuf.at[z, x, c, :, GU:WT]), (on_ref, wo.at[t, 0:V_A, :]), (ow_ref, wo.at[t, V_A:VD, :]),
        (res_hbm.at[pl.ds(pl.multiple_of(t * QUART, QUART), QUART), :], resq.at[:, my_cols]),
        (g1_ref, gfull.at[0, :, my_cols]), (b1_ref, gfull.at[1, :, my_cols]),
    ]
    local = [pltpu.make_async_copy(src, dst, ls.at[i]) for i, (src, dst) in enumerate(local)]
    for o in local:
        o.start()
    for o in local[:9]:
        o.wait()

    quarter = lax.broadcasted_iota(jnp.int32, (8, ROWS), 0)
    at = lax.broadcasted_iota(jnp.int32, (8, ROWS), 1)
    freq = jnp.ones((8, ROWS), F32)
    for i in range(1, 8):
        freq = jnp.where(quarter == i, THETA ** (-2.0 * i / 16), freq)
    row_angle = (s * (ROWS // GRID_W) + at // GRID_W).astype(F32) * freq
    col_angle = (at % GRID_W).astype(F32) * freq
    tab = (jnp.cos(row_angle), jnp.sin(row_angle), jnp.cos(col_angle), jnp.sin(col_angle))
    latent = root_scale(sl_ref[...], lg_ref[...]).astype(BF16)
    turned = turn(rk_ref[...].astype(F32), tab)
    for q in range(NY):
        kvbuf[z, c, q, 0:64, :] = latent[q * 64 : (q + 1) * 64]
        kvbuf[z, c, q, 64:80, :] = jnp.concatenate([turned[q * 8 : (q + 1) * 8], jnp.zeros((8, ROWS), F32)], axis=0).astype(BF16)
    qn = root_scale(ql_ref[...], qg_ref[...]).astype(BF16)
    narrow = dot(wqn_ref[...], qn, ((1,), (1,)))
    wide = dot(wqw_ref[...], qn, ((1,), (1,)))
    qbuf[x, 0:96, :] = jnp.concatenate([narrow[0:NOPE_A], turn(narrow[NOPE_A:], tab)], axis=0).astype(BF16)
    qbuf[x, 224:384, :] = jnp.concatenate([turn(wide[NOPE_B:], tab), wide[0:NOPE_B]], axis=0).astype(BF16)
    for j in range(NX):
        qbuf[j, 96:224, :] = jnp.zeros((128, ROWS), BF16)
    wk[:, 0:64] = kn_ref[...].T
    wk[:, 64:128] = jnp.zeros((LAT, 64), BF16)
    wk[:, 128:256] = kw_ref[...]
    wv[0:V_A, :] = vn_ref[...]
    wv[V_A:VD, :] = vw_ref[...].T

    pl.semaphore_wait(barrier, len(friends))

    send(kvbuf.at[z, c, t], kvbuf.at[z, c, t], M["KM"] + 1, dev_z(-1))
    send(kvbuf.at[z, c, t], kvbuf.at[z, c, t], M["KP"] + 1, dev_z(1))
    send(kvbuf.at[z, c], kvbuf.at[z, c], M["KT"], partner)
    for j in (2, 1, 3):
        for half, rows in enumerate((slice(0, 96), slice(224, 384))):
            send(qbuf.at[x, rows, :], qbuf.at[x, rows, :], M["Q"] + (j - 1) * 2 + half, dev_x(j))
    for o in local[9:12]:
        o.wait()

    def to_partner(u, zi, way):
        xi = at_x((0, -1, 1, 2)[way])
        send(b_slot(zi, xi), b_slot(zi, xi), M["PB"] + 4 * u + way, partner)

    def row_to_partner(u, zi):
        send(a_row(zi), a_row(zi), M["PA"] + u, partner)

    def to_x(u, zi):
        send(b_slot(zi, x), b_slot(zi, x), M["XP"] + u, dev_x(1))
        send(b_slot(zi, x), b_slot(zi, x), M["XM"] + u, dev_x(-1))

    def send_rows(zi, d, r):
        slot = a_slot(zi, at_x(-r))
        send(slot, slot, M["AP"] + 4 * d + r, dev_z(1))
        send(slot, slot, M["AM"] + 4 * d + r, dev_z(-1))

    def start_a():
        send_rows(z, 1, 0)
        for j in (2, 1, 3):
            send(a_slot(z, x), a_slot(z, x), M["A1"] + j, dev_x(j))

    def start_b():
        send(b_slot(z, x), b_slot(z, x), M["BM"] + 1, dev_z(-1))
        send(b_slot(z, x), b_slot(z, x), M["BP"] + 1, dev_z(1))
        to_partner(0, z, 0)

    def start_rows(*rs):
        for r in rs:
            arrived(a_slot(z, at_x(-r)), M["A1"] + r)
            send_rows(z, 1, r)
        if 2 in rs:
            row_to_partner(0, z)

    def rows_round(d, *rs):
        below, above = at_z(-d), at_z(d)
        for r in rs:
            if d < 4 or r < 2:
                arrived(a_slot(below, at_x(-r)), M["AP"] + 4 * d + r)
            if d < 3 or d == 3 and r < 2:
                send(a_slot(below, at_x(-r)), a_slot(below, at_x(-r)), M["AP"] + 4 * d + 4 + r, dev_z(1))
            if d < 4 or r >= 2:
                arrived(a_slot(above, at_x(-r)), M["AM"] + 4 * d + r)
            if d < 3 or d == 3 and r >= 2:
                send(a_slot(above, at_x(-r)), a_slot(above, at_x(-r)), M["AM"] + 4 * d + 4 + r, dev_z(-1))
            if r == 2:
                row_to_partner(2 * d - 1, below)
                if d < 4:
                    row_to_partner(2 * d, above)

    def slots_round(d, sideways=True):
        up, low = 2 * d - d // 4, 2 * d - 1
        arrived(b_slot(at_z(d), x), M["BM"] + d)
        if d < 4:
            send(b_slot(at_z(d), x), b_slot(at_z(d), x), M["BM"] + d + 1, dev_z(-1))
        to_partner(up, at_z(d), 0)
        if sideways:
            to_x(up, at_z(d))
        if d < 4:
            arrived(b_slot(at_z(-d), x), M["BP"] + d)
            if d < 3:
                send(b_slot(at_z(-d), x), b_slot(at_z(-d), x), M["BP"] + d + 1, dev_z(1))
            to_partner(low, at_z(-d), 0)
            if sideways:
                to_x(low, at_z(-d))

    plus = (0, 1, 3, 5)

    def part(u, zi, xi, way):
        slot = b_slot(zi, xi)
        return slot.at[pl.ds(way * SLOT // 2, SLOT // 2), :] if u == 7 else slot

    def relay(u):
        zu = zz(u)
        arrived(b_slot(zu, at_x(-1)), M["XP"] + u)
        if u in plus or u == 7:
            send(part(u, zu, at_x(-1), 0), part(u, zu, at_x(-1), 0), M["RL"] + u, dev_x(1))
        to_partner(u, zu, 1)
        arrived(b_slot(zu, at_x(1)), M["XM"] + u)
        if u not in plus:
            i = u + 1 if u == 7 else u
            send(part(u, zu, at_x(1), 1), part(u, zu, at_x(1), 1), M["RL"] + i, dev_x(-1))
        to_partner(u, zu, 2)

    def across(u):
        last = isinstance(u, int) and u == 7
        for way in range(2 if last else 1):
            arrived(part(7 if last else 0, zz(u), at_x(2), way), M["RL"] + u + way)
        to_partner(u, zz(u), 3)

    def partner_block(u):
        for way in range(4):
            arrived(wbuf.at[zz(u), at_x((0, -1, 1, 2)[way]), 1 - c, :, B_COLS], M["PB"] + 4 * u + way)

    start_b()
    start_a()
    to_x(0, z)
    wo_half = lambda core: pl.ds(pl.multiple_of(core * (D // 2), D // 2), D // 2)

    def send_wo():
        for j in (2, 1, 3):
            rows = pl.ds(pl.multiple_of(at_y(j) * QUART, QUART), QUART)
            send(res_hbm.at[rows, :], resq.at[:, my_cols], M["RS"] + j, dev_y(j))
            send(g1_ref, gfull.at[0, :, my_cols], M["GN"] + j, dev_y(j))
            send(b1_ref, gfull.at[1, :, my_cols], M["GN"] + 4 + j, dev_y(j))
        for j in (2, 1, 3):
            send(on_ref.at[:, wo_half(c)], wo.at[t, 0:V_A, wo_half(c)], M["WO"] + (j - 1) * 2, dev_y(j))
            send(ow_ref.at[:, wo_half(c)], wo.at[t, V_A:VD, wo_half(c)], M["WO"] + (j - 1) * 2 + 1, dev_y(j))

    def wo_across():
        for j in range(1, NY):
            arrived(wo.at[at_y(-j), 0:V_A, wo_half(c)], M["WO"] + (j - 1) * 2)
            arrived(wo.at[at_y(-j), V_A:VD, wo_half(c)], M["WO"] + (j - 1) * 2 + 1)
            send(wo.at[at_y(-j), :, wo_half(c)], wo.at[at_y(-j), :, wo_half(c)], M["WP"] + j, partner)

    for j in range(NX):
        ml[j] = jnp.concatenate([jnp.full((2, ROWS), -jnp.inf, F32), jnp.zeros((6, ROWS), F32)], axis=0)
        acc[j] = jnp.zeros((VD, ROWS), F32)

    def keys_of(zs):
        lane = lax.broadcasted_iota(jnp.int32, (ROWS, 128), 1)
        for core in range(2):
            latent = kvbuf[zs, core, :, 0:64, :].reshape(ROWS, LAT)
            turned = jnp.concatenate([kvbuf[zs, core, q, 64:80, :].astype(F32)[0:8] for q in range(NY)], axis=0)
            rot = jnp.concatenate([jnp.zeros((64, ROWS), F32), turned, turned], axis=0).T
            keys = dot(latent, wk[...], ((1,), (0,)))
            at = slice(core * ROWS, (core + 1) * ROWS)
            kx[at, 0:128] = jnp.where(lane < 64, keys[:, 0:128], rot).astype(BF16)
            kx[at, 128:256] = rot.astype(BF16)
            kx[at, 256:384] = keys[:, 128:256].astype(BF16)
            vx[:, at] = dot(wv[...], latent, ((1,), (1,))).astype(BF16)

    def attend(zs):
        keys_of(zs)

        heads = ((0, 128, 0, V_A, C_A), (128, 384, V_A, VD, C_B))
        every_score = [
            [dot(kx[:, lo:hi], qbuf[j, lo:hi, :], ((1,), (0,))) for lo, hi, _, _, _ in heads] for j in range(NX)
        ]
        for j in range(NX):
            for h, (_, _, vlo, vhi, scale) in enumerate(heads):
                scores = every_score[j][h]
                old = ml[j, h : h + 1, :]
                new = jnp.maximum(old, jnp.max(scores, axis=0, keepdims=True))
                factor = jnp.exp2((old - new) * scale)
                raised = jnp.exp2((scores - new) * scale).astype(BF16)
                ml[j, h : h + 1, :] = new
                with_ones = jnp.concatenate([vx[vlo:vhi, :], jnp.ones((16, 2 * ROWS), BF16)], axis=0)
                product = dot(with_ones, raised, ((1,), (0,)))
                ml[j, 2 + h : 3 + h, :] = ml[j, 2 + h : 3 + h, :] * factor + product[vhi - vlo : vhi - vlo + 1]
                acc[j, vlo:vhi, :] = acc[j, vlo:vhi, :] * factor + product[0 : vhi - vlo]

    def quarter_out(u):
        d, upwards = (u + 1) // 2, u % 2 and u != 7
        slot = kvbuf.at[zz(u), c, t]
        first = M["KP"] if upwards else M["KM"]
        arrived(slot, first + d)
        if d < (3 if upwards else 4):
            send(slot, slot, first + d + 1, dev_z(1 if upwards else -1))
        for j in (2, 1, 3):
            send(slot, slot, M["KY"] + 3 * u + j - 1, dev_y(j))

    def latents_across(u):
        zu = zz(u)
        for j in range(1, NY):
            arrived(kvbuf.at[zu, c, at_y(-j)], M["KY"] + 3 * u + j - 1)
        send(kvbuf.at[zu, c], kvbuf.at[zu, c], M["KT"] + u, partner)

    def on_step(k, value, then):
        @pl.when(k == value)
        def _():
            then()

    def unit(i, carry):
        @pl.when(i == 0)
        def _():
            for u in range(1, 5):
                quarter_out(u)
            for j in range(1, NX):
                for half, rows in enumerate((slice(0, 96), slice(224, 384))):
                    arrived(qbuf.at[at_x(-j), rows, :], M["Q"] + (j - 1) * 2 + half)

        on_step(i, 1, lambda: (quarter_out(5), quarter_out(6), slots_round(1)))
        on_step(i, 2, lambda: (quarter_out(7), send_wo(), start_rows(1)))
        on_step(i, 3, lambda: rows_round(1, 0))
        on_step(i, 4, lambda: slots_round(2))
        on_step(i, 5, lambda: start_rows(3, 2))
        on_step(i, 6, lambda: rows_round(1, 1))

        @pl.when(i < 7)
        def _():
            latents_across(i + 1)

        zi = zz(i)
        arrived(kvbuf.at[zi, 1 - c], M["KT"] + i)
        attend(zi)
        return carry

    lax.fori_loop(0, NZ, unit, 0)

    for j in range(NX):
        for h, (vlo, vhi) in enumerate(((0, V_A), (V_A, VD))):
            osend[j, vlo:vhi, :] = (acc[j, vlo:vhi, :] / ml[j, 2 + h : 3 + h, :]).astype(BF16)
    for j in (2, 1, 3):
        send(osend.at[at_x(j)], orecv.at[j - 1], M["O"] + j, dev_x(j))
        send(ml.at[at_x(j)], srecv.at[j - 1], M["OS"] + j, dev_x(j))

    relay(0)
    slots_round(3)
    relay(1)
    rows_round(1, 3)
    for j in range(1, NX):
        arrived(orecv.at[j - 1], M["O"] + j)
        arrived(srecv.at[j - 1], M["OS"] + j)
    for h, (vlo, vhi, scale) in enumerate(((0, V_A, C_A), (V_A, VD, C_B))):
        tops = [ml[x, h : h + 1, :]] + [srecv[j, h : h + 1, :] for j in range(3)]
        sums = [ml[x, 2 + h : 3 + h, :]] + [srecv[j, 2 + h : 3 + h, :] for j in range(3)]
        parts = [osend[x, vlo:vhi, :]] + [orecv[j, vlo:vhi, :] for j in range(3)]
        top = jnp.maximum(jnp.maximum(tops[0], tops[1]), jnp.maximum(tops[2], tops[3]))
        shares = [total * jnp.exp2((m - top) * scale) for m, total in zip(tops, sums)]
        total = shares[0] + shares[1] + shares[2] + shares[3]
        mixed = sum(part.astype(F32) * (share / total) for part, share in zip(parts, shares))
        attended[vlo:vhi, :] = mixed
    mine = attended[...].T.astype(BF16)
    for q in range(NY):
        attsend[q] = mine[q * QUART : (q + 1) * QUART]
    for j in (2, 1, 3):
        send(attsend.at[at_y(j)], att.at[t], M["AT"] + j, dev_y(j))

    wo_across()
    relay(2)
    relay(3)
    rows_round(1, 2)
    rows_round(2, 0)
    relay(4)
    rows_round(2, 1)

    for o in local[12:]:
        o.wait()
    for j in range(1, NY):
        arrived(resq.at[:, pl.ds(pl.multiple_of(at_y(-j) * DW, DW), DW)], M["RS"] + j)
        arrived(gfull.at[0, :, pl.ds(pl.multiple_of(at_y(-j) * DW, DW), DW)], M["GN"] + j)
        arrived(gfull.at[1, :, pl.ds(pl.multiple_of(at_y(-j) * DW, DW), DW)], M["GN"] + 4 + j)
        arrived(wo.at[at_y(-j), :, wo_half(1 - c)], M["WP"] + j)
    for j in range(1, NY):
        arrived(att.at[at_y(-j)], M["AT"] + j)

    def norm(stat, got, first, gain_ref, bias_ref):
        h = hres[...]
        center = jnp.mean(h, axis=1, keepdims=True)
        apart = jnp.sum((h - center) * (h - center), axis=1, keepdims=True)
        lane = lax.broadcasted_iota(jnp.int32, (ROWS, 128), 1)
        both = jnp.where(lane == 0, center, jnp.where(lane == 1, apart, 0.0))
        stat[...] = both.T[0:8]
        for j in (2, 1, 3):
            send(stat, got.at[j - 1], first + j, dev_y(j))
        for j in range(1, NY):
            arrived(got.at[j - 1], first + j)
        centers = [stat[0:1, :]] + [got[j, 0:1, :] for j in range(3)]
        aparts = [stat[1:2, :]] + [got[j, 1:2, :] for j in range(3)]
        middle = (centers[0] + centers[1] + centers[2] + centers[3]) * 0.25
        spread = sum(aparts) + DW * sum((m - middle) * (m - middle) for m in centers)
        root = lax.rsqrt(spread * (1.0 / D) + EPS_LAYER)
        cols = jnp.concatenate([middle, root, jnp.zeros((126, ROWS), F32)], axis=0).T
        return ((h - cols[:, 0:1]) * cols[:, 1:2] * gain_ref[...] + bias_ref[...]).astype(BF16)

    h = DEEP_ALPHA * resq[...].astype(F32) + dot(attsend[t], wo[t], ((1,), (0,)))
    for j in range(1, NY):
        h = h + dot(att[at_y(j)], wo[at_y(j)], ((1,), (0,)))
    center = jnp.mean(h, axis=1, keepdims=True)
    spread = jnp.mean((h - center) * (h - center), axis=1, keepdims=True)
    my_rows = pl.ds(pl.multiple_of(t * QUART, QUART), QUART)
    xbuf[my_rows, :] = ((h - center) * lax.rsqrt(spread + EPS_LAYER) * gfull[0] + gfull[1]).astype(BF16)

    def x_half(off, half):
        return xbuf.at[pl.ds(pl.multiple_of(at_y(off) * QUART, QUART), QUART), pl.ds(half * (D // 2), D // 2)]

    def send_x(off, half, i, way):
        send(x_half(off, half), x_half(off, half), M["G"] + i, dev_y(way))

    for i, half, way in ((0, 0, 1), (2, 1, -1), (1, 1, 1), (3, 0, -1)):
        send_x(0, half, i, way)
    slots_round(4)
    relay(5)
    arrived(x_half(-1, 0), M["G"])
    send_x(-1, 0, 4, 1)
    arrived(x_half(1, 1), M["G"] + 2)
    send_x(1, 1, 5, -1)
    rows_round(2, 3, 2)
    relay(6)
    across(0)
    across(1)
    rows_round(3, 0)
    across(2)
    rows_round(3, 1)
    across(3)
    relay(7)
    rows_round(3, 3, 2)
    for i, off, half in ((1, -1, 1), (3, 1, 0), (4, 2, 0), (5, 2, 1)):
        arrived(x_half(off, half), M["G"] + i)

    hres[...] = DEEP_ALPHA * xbuf[:, my_cols].astype(F32)

    def gate_up(u):
        zu = zz(u)
        features = xbuf[:, pl.ds(pl.multiple_of(zu * 256, 256), 256)]
        for n in range(GU // 256):
            cols = slice(n * 256, (n + 1) * 256)
            part = dot(features, wbuf[zu, :, :, :, cols].reshape(256, 256), ((1,), (0,)))
            gbuf[:, cols] = part if isinstance(u, int) else gbuf[:, cols] + part

    def partner_rows(u):
        arrived(wbuf.at[zz(u), :, 1 - c, :, A_COLS], M["PA"] + u)

    partner_block(0)
    partner_rows(0)
    gate_up(0)

    def block(u, carry):
        @pl.when(u <= 3)
        def _():
            across(u + 3)

        on_step(u, 4, lambda: across(7))
        on_step(u, 5, lambda: rows_round(4, 0, 1, 3, 2))

        partner_block(u)
        partner_rows(u)
        gate_up(u)
        return carry

    lax.fori_loop(1, NZ, block, 0)
    gate = gbuf[:, 0:FH]
    hid[...] = (gate / (1.0 + jnp.exp(-gate)) * gbuf[:, FH:GU]).astype(BF16)

    def feed(off):
        return dot(hid[...], wbuf[pl.ds(at_y(off) * 2, 2), :, :, :, GU:WT].reshape(DW, FH), ((1,), (1,)))

    first, second = slice(0, HALF), slice(HALF, ROWS)
    fsend[1] = feed(2).astype(BF16)
    send(fsend.at[1, first], fthru.at[0], M["F"], dev_y(1))
    send(fsend.at[1, second], fthru.at[1], M["F"] + 1, dev_y(-1))
    after = feed(1)
    fsend[0, second] = after[second].astype(BF16)
    send(fsend.at[0, second], frecv.at[0, second], M["F"] + 2, dev_y(1))
    fkeep[0] = after[first]
    before = feed(3)
    fsend[2, first] = before[first].astype(BF16)
    send(fsend.at[2, first], frecv.at[1, first], M["F"] + 3, dev_y(-1))
    fkeep[1] = before[second]
    arrived(fthru.at[0], M["F"])
    fsend[0, first] = (fkeep[0] + fthru[0].astype(F32)).astype(BF16)
    send(fsend.at[0, first], frecv.at[0, first], M["F"] + 4, dev_y(1))
    arrived(fthru.at[1], M["F"] + 1)
    fsend[2, second] = (fkeep[1] + fthru[1].astype(F32)).astype(BF16)
    send(fsend.at[2, second], frecv.at[1, second], M["F"] + 5, dev_y(-1))
    for j in range(1, NX):
        sent(qbuf.at[0, 0:96, :], M["Q"] + (j - 1) * 2)
        sent(qbuf.at[0, 224:384, :], M["Q"] + (j - 1) * 2 + 1)
        sent(a_slot(0, 0), M["A1"] + j)
        sent(osend.at[0], M["O"] + j)
        sent(ml.at[0], M["OS"] + j)
        sent(wo.at[0, 0:V_A, wo_half(0)], M["WO"] + (j - 1) * 2)
        sent(wo.at[0, V_A:VD, wo_half(0)], M["WO"] + (j - 1) * 2 + 1)
        sent(wo.at[0, :, wo_half(0)], M["WP"] + j)
        sent(resq.at[:, my_cols], M["RS"] + j)
        sent(g1_ref, M["GN"] + j)
        sent(b1_ref, M["GN"] + 4 + j)
        sent(att.at[0], M["AT"] + j)
    for d in range(1, 5):
        for way in "MP":
            for r in range(4):
                if d < 4 or (r >= 2) == (way == "M"):
                    sent(a_slot(0, 0), M["A" + way] + 4 * d + r)
            if d < 4 or way == "M":
                sent(b_slot(0, 0), M["B" + way] + d)
    for u in range(NZ):
        sent(kvbuf.at[0, 0], M["KT"] + u)
        if u > 0:
            sent(kvbuf.at[0, 0, 0], M["KM"] + u if u < 5 else M["KP"] + u - 4)
            for j in range(1, NY):
                sent(kvbuf.at[0, 0, 0], M["KY"] + 3 * u + j - 1)
        sent(a_row(0), M["PA"] + u)
        for way in range(4):
            sent(b_slot(0, 0), M["PB"] + 4 * u + way)
        for name in ("XP", "XM"):
            sent(b_slot(0, 0), M[name] + u)
        sent(part(u, 0, 0, 0), M["RL"] + u)
    sent(part(7, 0, 0, 1), M["RL"] + 8)
    for i in range(6):
        sent(x_half(0, 0), M["G"] + i)
    hres[...] += feed(0)
    for i, k, rows in ((2, 0, second), (3, 1, first), (4, 0, first), (5, 1, second)):
        arrived(frecv.at[k, rows], M["F"] + i)
    hres[...] += frecv[0].astype(F32) + frecv[1].astype(F32)
    out_ref[...] = norm(st2, sr2, M["S2"], g2_ref, b2_ref)

    for j in range(1, NX):
        sent(st2, M["S2"] + j)
    for i in range(6):
        sent(fsend.at[0, 0:HALF], M["F"] + i)


def body(
    residual, query_latent, shared_latent, rotary_key, query_gain, latent_gain, query_narrow, key_narrow,
    value_narrow, query_wide, key_wide, value_wide, output_narrow, output_wide, first_gain, first_bias,
    gate_weight, up_weight, down_weight, second_gain, second_bias,
):
    row = lambda v: v.reshape(1, -1)
    large = (
        residual, query_latent, shared_latent, rotary_key.T, query_narrow.T, key_narrow.T, value_narrow.T,
        query_wide.T, key_wide, value_wide, output_narrow, output_wide, gate_weight, up_weight, down_weight.T,
    )
    small = (
        row(query_gain), row(latent_gain), row(first_gain), row(first_bias), row(second_gain), row(second_bias),
    )
    vmem = pl.BlockSpec(memory_space=pltpu.VMEM)
    return pl.pallas_call(
        layer_kernel,
        out_shape=jax.ShapeDtypeStruct((ROWS, DW), BF16),
        in_specs=[pl.BlockSpec(memory_space=pl.ANY)] * len(large) + [vmem] * len(small),
        out_specs=vmem,
        scratch_shapes=[
            *[pltpu.VMEM(v.shape, v.dtype) for v in large[1:10]],
            pltpu.VMEM((NZ, 2, NY, 80, LAT), BF16),
            pltpu.VMEM((NX, KX, ROWS), BF16),
            pltpu.VMEM((NZ, NX, 2, SLOT, WT), BF16),
            pltpu.VMEM((LAT, 256), BF16),
            pltpu.VMEM((VD, LAT), BF16),
            pltpu.VMEM((2 * ROWS, KX), BF16),
            pltpu.VMEM((VD, 2 * ROWS), BF16),
            pltpu.VMEM((NX, 8, ROWS), F32),
            pltpu.VMEM((NX, VD, ROWS), F32),
            pltpu.VMEM((NX, VD, ROWS), BF16),
            pltpu.VMEM((3, VD, ROWS), BF16),
            pltpu.VMEM((3, 8, ROWS), F32),
            pltpu.VMEM((VD, ROWS), F32),
            pltpu.VMEM((NY, QUART, VD), BF16),
            pltpu.VMEM((NY, QUART, VD), BF16),
            pltpu.VMEM((NY, VD, D), BF16),
            pltpu.VMEM((QUART, D), BF16),
            pltpu.VMEM((2, 1, D), F32),
            pltpu.VMEM((8, ROWS), F32),
            pltpu.VMEM((3, 8, ROWS), F32),
            pltpu.VMEM((ROWS, D), BF16),
            pltpu.VMEM((ROWS, GU), F32),
            pltpu.VMEM((ROWS, FH), BF16),
            pltpu.VMEM((3, ROWS, DW), BF16),
            pltpu.VMEM((2, ROWS, DW), BF16),
            pltpu.VMEM((2, HALF, DW), BF16),
            pltpu.VMEM((2, HALF, DW), F32),
            pltpu.VMEM((ROWS, DW), F32),
            pltpu.SemaphoreType.DMA((MESSAGES,)),
            pltpu.SemaphoreType.DMA((MESSAGES,)),
            pltpu.SemaphoreType.DMA((len(large) + 2,)),
        ],
        compiler_params=pltpu.CompilerParams(
            collective_id=0, has_side_effects=True, vmem_limit_bytes=60 * 1024 * 1024
        ),
    )(*large, *small)


def solution(mesh):
    return jax.shard_map(
        body,
        mesh=mesh,
        in_specs=(
            P("sp", "tp"),
            P("sp", None),
            P("sp", None),
            P("sp", None),
            P(),
            P(),
            P(None, "tp"),
            P(None, "tp"),
            P(None, "tp"),
            P(None, "tp"),
            P(None, "tp"),
            P(None, "tp"),
            P("tp", None),
            P("tp", None),
            P("tp"),
            P("tp"),
            P("sp", "tp"),
            P("sp", "tp"),
            P("tp", "sp"),
            P("tp"),
            P("tp"),
        ),
        out_specs=P("sp", "tp"),
        check_vma=False,
    )
```

```python
import jax
import jax.numpy as jnp
from jax import lax
from jax.experimental import pallas as pl
from jax.experimental.pallas import tpu as pltpu
from jax.sharding import PartitionSpec as P

ROPE = 32
NOPE_A = 64
V_A = 64
NOPE_B = 128
V_B = 128
GRID_W = 64
EPS_ROOT = 1e-06
EPS_LAYER = 1e-05
THETA = 10000.0
DEEP_ALPHA = 2.0**0.25
LOG2E = 1.4426950408889634

NZ, NX, NY = 8, 4, 4
ROWS = 256
HALF = ROWS // 2
QUART = ROWS // 4
LAT = 256
DW = 512
D = 2048
FH = 1408
GU = 2 * FH
WT = 3 * FH
WB = GU - 512
B_COLS, A_COLS = slice(0, WB), slice(WB, WT)
SLOT = 32
VD = V_A + V_B
KX = 128 + 256
C_A = (NOPE_A + ROPE) ** -0.5 * LOG2E
C_B = (NOPE_B + ROPE) ** -0.5 * LOG2E
MESH = pl.DeviceIdType.MESH
F32, BF16 = jnp.float32, jnp.bfloat16


def numbered(**counts):
    at, table = 0, {}
    for name, count in counts.items():
        table[name] = at
        at += count
    return table, at


M, MESSAGES = numbered(
    Q=6, KM=5, KP=4, KY=24, KT=8, O=4, OS=4, WO=6, WP=4, RS=4, GN=8, AT=4, G=6, F=6, S2=4,
    A1=4, AM=20, AP=20, BM=5, BP=4, XP=8, XM=8, RL=9, PB=32, PA=8,
)


def dot(a, b, dims):
    return lax.dot_general(a, b, (dims, ((), ())), preferred_element_type=F32)


def root_scale(latent, gain):
    x = latent.astype(F32)
    return x * lax.rsqrt(jnp.mean(x * x, axis=-1, keepdims=True) + EPS_ROOT) * gain


def turn(v, tab):
    cr, sr, cc, sc = tab
    a, b, c, d = v[0:8], v[8:16], v[16:24], v[24:32]
    return jnp.concatenate([a * cr - b * sr, b * cr + a * sr, c * cc - d * sc, d * cc + c * sc], axis=0)


def layer_kernel(
    res_hbm, ql_hbm, sl_hbm, rk_hbm, wqn_hbm, kn_hbm, vn_hbm, wqw_hbm, kw_hbm, vw_hbm, on_ref, ow_ref,
    gate_ref, up_ref, down_ref, qg_ref, lg_ref, g1_ref, b1_ref, g2_ref, b2_ref,
    out_ref,
    ql_ref, sl_ref, rk_ref, wqn_ref, kn_ref, vn_ref, wqw_ref, kw_ref, vw_ref,
    kvbuf, qbuf, wbuf, wk, wv, kx, vx, ml, acc, osend, orecv, srecv, attended, attsend, att, wo, resq, gfull, st2, sr2,
    xbuf, gbuf, hid, fsend, frecv, fthru, fkeep, hres, ss, rs, ls,
):
    s, t = lax.axis_index("sp"), lax.axis_index("tp")
    c = lax.rem(s, 2)
    x = lax.rem(lax.div(s, 2), NX)
    z = lax.div(s, 2 * NX)

    def at_z(off):
        return lax.rem(z + off + NZ, NZ)

    def at_x(off):
        return lax.rem(x + off + NX, NX)

    def at_y(off):
        return lax.rem(t + off + NY, NY)

    def dev_z(off):
        return (at_z(off) * (2 * NX) + x * 2 + c, t)

    def dev_x(off):
        return (z * (2 * NX) + at_x(off) * 2 + c, t)

    def dev_y(off):
        return (s, at_y(off))

    partner = (s + 1 - 2 * c, t)

    def zz(u):
        return at_z(lax.div(u + 1, 2) * (1 - 2 * lax.rem(u, 2)) if not isinstance(u, int) else (u + 1) // 2 * (1 - 2 * (u % 2)))


    def msg(src, dst, i, dev):
        return pltpu.make_async_remote_copy(
            src_ref=src, dst_ref=dst, send_sem=ss.at[i], recv_sem=rs.at[i],
            device_id=dev, device_id_type=MESH,
        )

    def send(src, dst, i, dev):
        msg(src, dst, i, dev).start()

    def arrived(dst, i):
        msg(dst, dst, i, partner).wait_recv()

    def sent(src, i):
        msg(src, src, i, partner).wait_send()

    b_slot = lambda zi, xi: wbuf.at[zi, xi, c, :, B_COLS]
    a_slot = lambda zi, xi: wbuf.at[zi, xi, c, :, A_COLS]
    a_row = lambda zi: wbuf.at[zi, :, c, :, A_COLS]

    barrier = pltpu.get_barrier_semaphore()
    friends = [dev_z(1), dev_z(-1), dev_x(1), dev_x(2), dev_x(3), partner, dev_y(1), dev_y(2), dev_y(3)]
    for f in friends:
        pl.semaphore_signal(barrier, inc=1, device_id=f, device_id_type=MESH)

    my_cols = pl.ds(pl.multiple_of(t * DW, DW), DW)
    local = [
        (sl_hbm, sl_ref), (rk_hbm, rk_ref), (ql_hbm, ql_ref), (wqn_hbm, wqn_ref), (wqw_hbm, wqw_ref),
        (kn_hbm, kn_ref), (kw_hbm, kw_ref), (vn_hbm, vn_ref), (vw_hbm, vw_ref),
        (gate_ref, wbuf.at[z, x, c, :, 0:FH]), (up_ref, wbuf.at[z, x, c, :, FH:GU]),
        (down_ref, wbuf.at[z, x, c, :, GU:WT]), (on_ref, wo.at[t, 0:V_A, :]), (ow_ref, wo.at[t, V_A:VD, :]),
        (res_hbm.at[pl.ds(pl.multiple_of(t * QUART, QUART), QUART), :], resq.at[:, my_cols]),
        (g1_ref, gfull.at[0, :, my_cols]), (b1_ref, gfull.at[1, :, my_cols]),
    ]
    local = [pltpu.make_async_copy(src, dst, ls.at[i]) for i, (src, dst) in enumerate(local)]
    for o in local:
        o.start()
    for o in local[:9]:
        o.wait()

    quarter = lax.broadcasted_iota(jnp.int32, (8, ROWS), 0)
    at = lax.broadcasted_iota(jnp.int32, (8, ROWS), 1)
    freq = jnp.ones((8, ROWS), F32)
    for i in range(1, 8):
        freq = jnp.where(quarter == i, THETA ** (-2.0 * i / 16), freq)
    row_angle = (s * (ROWS // GRID_W) + at // GRID_W).astype(F32) * freq
    col_angle = (at % GRID_W).astype(F32) * freq
    tab = (jnp.cos(row_angle), jnp.sin(row_angle), jnp.cos(col_angle), jnp.sin(col_angle))
    latent = root_scale(sl_ref[...], lg_ref[...]).astype(BF16)
    turned = turn(rk_ref[...].astype(F32), tab)
    for q in range(NY):
        kvbuf[z, c, q, 0:64, :] = latent[q * 64 : (q + 1) * 64]
        kvbuf[z, c, q, 64:80, :] = jnp.concatenate([turned[q * 8 : (q + 1) * 8], jnp.zeros((8, ROWS), F32)], axis=0).astype(BF16)
    qn = root_scale(ql_ref[...], qg_ref[...]).astype(BF16)
    narrow = dot(wqn_ref[...], qn, ((1,), (1,)))
    wide = dot(wqw_ref[...], qn, ((1,), (1,)))
    qbuf[x, 0:96, :] = jnp.concatenate([narrow[0:NOPE_A], turn(narrow[NOPE_A:], tab)], axis=0).astype(BF16)
    qbuf[x, 224:384, :] = jnp.concatenate([turn(wide[NOPE_B:], tab), wide[0:NOPE_B]], axis=0).astype(BF16)
    for j in range(NX):
        qbuf[j, 96:224, :] = jnp.zeros((128, ROWS), BF16)
    wk[:, 0:64] = kn_ref[...].T
    wk[:, 64:128] = jnp.zeros((LAT, 64), BF16)
    wk[:, 128:256] = kw_ref[...]
    wv[0:V_A, :] = vn_ref[...]
    wv[V_A:VD, :] = vw_ref[...].T

    pl.semaphore_wait(barrier, len(friends))

    send(kvbuf.at[z, c, t], kvbuf.at[z, c, t], M["KM"] + 1, dev_z(-1))
    send(kvbuf.at[z, c, t], kvbuf.at[z, c, t], M["KP"] + 1, dev_z(1))
    send(kvbuf.at[z, c], kvbuf.at[z, c], M["KT"], partner)
    for j in (2, 1, 3):
        for half, rows in enumerate((slice(0, 96), slice(224, 384))):
            send(qbuf.at[x, rows, :], qbuf.at[x, rows, :], M["Q"] + (j - 1) * 2 + half, dev_x(j))
    for o in local[9:12]:
        o.wait()

    def to_partner(u, zi, way):
        xi = at_x((0, -1, 1, 2)[way])
        send(b_slot(zi, xi), b_slot(zi, xi), M["PB"] + 4 * u + way, partner)

    def row_to_partner(u, zi):
        send(a_row(zi), a_row(zi), M["PA"] + u, partner)

    def to_x(u, zi):
        send(b_slot(zi, x), b_slot(zi, x), M["XP"] + u, dev_x(1))
        send(b_slot(zi, x), b_slot(zi, x), M["XM"] + u, dev_x(-1))

    def send_rows(zi, d, r):
        slot = a_slot(zi, at_x(-r))
        send(slot, slot, M["AP"] + 4 * d + r, dev_z(1))
        send(slot, slot, M["AM"] + 4 * d + r, dev_z(-1))

    def start_a():
        send_rows(z, 1, 0)
        for j in (2, 1, 3):
            send(a_slot(z, x), a_slot(z, x), M["A1"] + j, dev_x(j))

    def start_b():
        send(b_slot(z, x), b_slot(z, x), M["BM"] + 1, dev_z(-1))
        send(b_slot(z, x), b_slot(z, x), M["BP"] + 1, dev_z(1))
        to_partner(0, z, 0)

    def start_rows(*rs):
        for r in rs:
            arrived(a_slot(z, at_x(-r)), M["A1"] + r)
            send_rows(z, 1, r)
        if 2 in rs:
            row_to_partner(0, z)

    def rows_round(d, *rs):
        below, above = at_z(-d), at_z(d)
        for r in rs:
            if d < 4 or r < 2:
                arrived(a_slot(below, at_x(-r)), M["AP"] + 4 * d + r)
            if d < 3 or d == 3 and r < 2:
                send(a_slot(below, at_x(-r)), a_slot(below, at_x(-r)), M["AP"] + 4 * d + 4 + r, dev_z(1))
            if d < 4 or r >= 2:
                arrived(a_slot(above, at_x(-r)), M["AM"] + 4 * d + r)
            if d < 3 or d == 3 and r >= 2:
                send(a_slot(above, at_x(-r)), a_slot(above, at_x(-r)), M["AM"] + 4 * d + 4 + r, dev_z(-1))
            if r == 2:
                row_to_partner(2 * d - 1, below)
                if d < 4:
                    row_to_partner(2 * d, above)

    def slots_round(d, sideways=True):
        up, low = 2 * d - d // 4, 2 * d - 1
        arrived(b_slot(at_z(d), x), M["BM"] + d)
        if d < 4:
            send(b_slot(at_z(d), x), b_slot(at_z(d), x), M["BM"] + d + 1, dev_z(-1))
        to_partner(up, at_z(d), 0)
        if sideways:
            to_x(up, at_z(d))
        if d < 4:
            arrived(b_slot(at_z(-d), x), M["BP"] + d)
            if d < 3:
                send(b_slot(at_z(-d), x), b_slot(at_z(-d), x), M["BP"] + d + 1, dev_z(1))
            to_partner(low, at_z(-d), 0)
            if sideways:
                to_x(low, at_z(-d))

    plus = (0, 1, 3, 5)

    def part(u, zi, xi, way):
        slot = b_slot(zi, xi)
        return slot.at[pl.ds(way * SLOT // 2, SLOT // 2), :] if u == 7 else slot

    def relay(u):
        zu = zz(u)
        arrived(b_slot(zu, at_x(-1)), M["XP"] + u)
        if u in plus or u == 7:
            send(part(u, zu, at_x(-1), 0), part(u, zu, at_x(-1), 0), M["RL"] + u, dev_x(1))
        to_partner(u, zu, 1)
        arrived(b_slot(zu, at_x(1)), M["XM"] + u)
        if u not in plus:
            i = u + 1 if u == 7 else u
            send(part(u, zu, at_x(1), 1), part(u, zu, at_x(1), 1), M["RL"] + i, dev_x(-1))
        to_partner(u, zu, 2)

    def across(u):
        last = isinstance(u, int) and u == 7
        for way in range(2 if last else 1):
            arrived(part(7 if last else 0, zz(u), at_x(2), way), M["RL"] + u + way)
        to_partner(u, zz(u), 3)

    def partner_block(u):
        for way in range(4):
            arrived(wbuf.at[zz(u), at_x((0, -1, 1, 2)[way]), 1 - c, :, B_COLS], M["PB"] + 4 * u + way)

    start_b()
    start_a()
    to_x(0, z)
    wo_half = lambda core: pl.ds(pl.multiple_of(core * (D // 2), D // 2), D // 2)

    def send_wo():
        for j in (2, 1, 3):
            rows = pl.ds(pl.multiple_of(at_y(j) * QUART, QUART), QUART)
            send(res_hbm.at[rows, :], resq.at[:, my_cols], M["RS"] + j, dev_y(j))
            send(g1_ref, gfull.at[0, :, my_cols], M["GN"] + j, dev_y(j))
            send(b1_ref, gfull.at[1, :, my_cols], M["GN"] + 4 + j, dev_y(j))
        for j in (2, 1, 3):
            send(on_ref.at[:, wo_half(c)], wo.at[t, 0:V_A, wo_half(c)], M["WO"] + (j - 1) * 2, dev_y(j))
            send(ow_ref.at[:, wo_half(c)], wo.at[t, V_A:VD, wo_half(c)], M["WO"] + (j - 1) * 2 + 1, dev_y(j))

    def wo_across():
        for j in range(1, NY):
            arrived(wo.at[at_y(-j), 0:V_A, wo_half(c)], M["WO"] + (j - 1) * 2)
            arrived(wo.at[at_y(-j), V_A:VD, wo_half(c)], M["WO"] + (j - 1) * 2 + 1)
            send(wo.at[at_y(-j), :, wo_half(c)], wo.at[at_y(-j), :, wo_half(c)], M["WP"] + j, partner)

    for j in range(NX):
        ml[j] = jnp.concatenate([jnp.full((2, ROWS), -jnp.inf, F32), jnp.zeros((6, ROWS), F32)], axis=0)
        acc[j] = jnp.zeros((VD, ROWS), F32)

    def keys_of(zs):
        lane = lax.broadcasted_iota(jnp.int32, (ROWS, 128), 1)
        for core in range(2):
            latent = kvbuf[zs, core, :, 0:64, :].reshape(ROWS, LAT)
            turned = jnp.concatenate([kvbuf[zs, core, q, 64:80, :].astype(F32)[0:8] for q in range(NY)], axis=0)
            rot = jnp.concatenate([jnp.zeros((64, ROWS), F32), turned, turned], axis=0).T
            keys = dot(latent, wk[...], ((1,), (0,)))
            at = slice(core * ROWS, (core + 1) * ROWS)
            kx[at, 0:128] = jnp.where(lane < 64, keys[:, 0:128], rot).astype(BF16)
            kx[at, 128:256] = rot.astype(BF16)
            kx[at, 256:384] = keys[:, 128:256].astype(BF16)
            vx[:, at] = dot(wv[...], latent, ((1,), (1,))).astype(BF16)

    def attend(zs):
        keys_of(zs)

        heads = ((0, 128, 0, V_A, C_A), (128, 384, V_A, VD, C_B))
        every_score = [
            [dot(kx[:, lo:hi], qbuf[j, lo:hi, :], ((1,), (0,))) for lo, hi, _, _, _ in heads] for j in range(NX)
        ]
        for j in range(NX):
            for h, (_, _, vlo, vhi, scale) in enumerate(heads):
                scores = every_score[j][h]
                old = ml[j, h : h + 1, :]
                new = jnp.maximum(old, jnp.max(scores, axis=0, keepdims=True))
                factor = jnp.exp2((old - new) * scale)
                raised = jnp.exp2((scores - new) * scale).astype(BF16)
                ml[j, h : h + 1, :] = new
                with_ones = jnp.concatenate([vx[vlo:vhi, :], jnp.ones((16, 2 * ROWS), BF16)], axis=0)
                product = dot(with_ones, raised, ((1,), (0,)))
                ml[j, 2 + h : 3 + h, :] = ml[j, 2 + h : 3 + h, :] * factor + product[vhi - vlo : vhi - vlo + 1]
                acc[j, vlo:vhi, :] = acc[j, vlo:vhi, :] * factor + product[0 : vhi - vlo]

    def quarter_out(u):
        d, upwards = (u + 1) // 2, u % 2 and u != 7
        slot = kvbuf.at[zz(u), c, t]
        first = M["KP"] if upwards else M["KM"]
        arrived(slot, first + d)
        if d < (3 if upwards else 4):
            send(slot, slot, first + d + 1, dev_z(1 if upwards else -1))
        for j in (2, 1, 3):
            send(slot, slot, M["KY"] + 3 * u + j - 1, dev_y(j))

    def latents_across(u):
        zu = zz(u)
        for j in range(1, NY):
            arrived(kvbuf.at[zu, c, at_y(-j)], M["KY"] + 3 * u + j - 1)
        send(kvbuf.at[zu, c], kvbuf.at[zu, c], M["KT"] + u, partner)

    def on_step(k, value, then):
        @pl.when(k == value)
        def _():
            then()

    def unit(i, carry):
        @pl.when(i == 0)
        def _():
            for u in range(1, 5):
                quarter_out(u)
            for j in range(1, NX):
                for half, rows in enumerate((slice(0, 96), slice(224, 384))):
                    arrived(qbuf.at[at_x(-j), rows, :], M["Q"] + (j - 1) * 2 + half)

        on_step(i, 1, lambda: (quarter_out(5), quarter_out(6), slots_round(1)))
        on_step(i, 2, lambda: (quarter_out(7), send_wo(), start_rows(1)))
        on_step(i, 3, lambda: rows_round(1, 0))
        on_step(i, 4, lambda: slots_round(2))
        on_step(i, 5, lambda: start_rows(3, 2))
        on_step(i, 6, lambda: rows_round(1, 1))

        @pl.when(i < 7)
        def _():
            latents_across(i + 1)

        zi = zz(i)
        arrived(kvbuf.at[zi, 1 - c], M["KT"] + i)
        attend(zi)
        return carry

    lax.fori_loop(0, NZ, unit, 0)

    for j in range(NX):
        for h, (vlo, vhi) in enumerate(((0, V_A), (V_A, VD))):
            osend[j, vlo:vhi, :] = (acc[j, vlo:vhi, :] / ml[j, 2 + h : 3 + h, :]).astype(BF16)
    for j in (2, 1, 3):
        send(osend.at[at_x(j)], orecv.at[j - 1], M["O"] + j, dev_x(j))
        send(ml.at[at_x(j)], srecv.at[j - 1], M["OS"] + j, dev_x(j))

    relay(0)
    slots_round(3)
    relay(1)
    rows_round(1, 3)
    for j in range(1, NX):
        arrived(orecv.at[j - 1], M["O"] + j)
        arrived(srecv.at[j - 1], M["OS"] + j)
    for h, (vlo, vhi, scale) in enumerate(((0, V_A, C_A), (V_A, VD, C_B))):
        tops = [ml[x, h : h + 1, :]] + [srecv[j, h : h + 1, :] for j in range(3)]
        sums = [ml[x, 2 + h : 3 + h, :]] + [srecv[j, 2 + h : 3 + h, :] for j in range(3)]
        parts = [osend[x, vlo:vhi, :]] + [orecv[j, vlo:vhi, :] for j in range(3)]
        top = jnp.maximum(jnp.maximum(tops[0], tops[1]), jnp.maximum(tops[2], tops[3]))
        shares = [total * jnp.exp2((m - top) * scale) for m, total in zip(tops, sums)]
        total = shares[0] + shares[1] + shares[2] + shares[3]
        mixed = sum(part.astype(F32) * (share / total) for part, share in zip(parts, shares))
        attended[vlo:vhi, :] = mixed
    mine = attended[...].T.astype(BF16)
    for q in range(NY):
        attsend[q] = mine[q * QUART : (q + 1) * QUART]
    for j in (2, 1, 3):
        send(attsend.at[at_y(j)], att.at[t], M["AT"] + j, dev_y(j))

    wo_across()
    relay(2)
    relay(3)
    rows_round(1, 2)
    rows_round(2, 0)
    relay(4)
    rows_round(2, 1)

    for o in local[12:]:
        o.wait()
    for j in range(1, NY):
        arrived(resq.at[:, pl.ds(pl.multiple_of(at_y(-j) * DW, DW), DW)], M["RS"] + j)
        arrived(gfull.at[0, :, pl.ds(pl.multiple_of(at_y(-j) * DW, DW), DW)], M["GN"] + j)
        arrived(gfull.at[1, :, pl.ds(pl.multiple_of(at_y(-j) * DW, DW), DW)], M["GN"] + 4 + j)
        arrived(wo.at[at_y(-j), :, wo_half(1 - c)], M["WP"] + j)
    for j in range(1, NY):
        arrived(att.at[at_y(-j)], M["AT"] + j)

    def norm(stat, got, first, gain_ref, bias_ref):
        h = hres[...]
        center = jnp.mean(h, axis=1, keepdims=True)
        apart = jnp.sum((h - center) * (h - center), axis=1, keepdims=True)
        lane = lax.broadcasted_iota(jnp.int32, (ROWS, 128), 1)
        both = jnp.where(lane == 0, center, jnp.where(lane == 1, apart, 0.0))
        stat[...] = both.T[0:8]
        for j in (2, 1, 3):
            send(stat, got.at[j - 1], first + j, dev_y(j))
        for j in range(1, NY):
            arrived(got.at[j - 1], first + j)
        centers = [stat[0:1, :]] + [got[j, 0:1, :] for j in range(3)]
        aparts = [stat[1:2, :]] + [got[j, 1:2, :] for j in range(3)]
        middle = (centers[0] + centers[1] + centers[2] + centers[3]) * 0.25
        spread = sum(aparts) + DW * sum((m - middle) * (m - middle) for m in centers)
        root = lax.rsqrt(spread * (1.0 / D) + EPS_LAYER)
        cols = jnp.concatenate([middle, root, jnp.zeros((126, ROWS), F32)], axis=0).T
        return ((h - cols[:, 0:1]) * cols[:, 1:2] * gain_ref[...] + bias_ref[...]).astype(BF16)

    h = DEEP_ALPHA * resq[...].astype(F32) + dot(attsend[t], wo[t], ((1,), (0,)))
    for j in range(1, NY):
        h = h + dot(att[at_y(j)], wo[at_y(j)], ((1,), (0,)))
    center = jnp.mean(h, axis=1, keepdims=True)
    spread = jnp.mean((h - center) * (h - center), axis=1, keepdims=True)
    my_rows = pl.ds(pl.multiple_of(t * QUART, QUART), QUART)
    xbuf[my_rows, :] = ((h - center) * lax.rsqrt(spread + EPS_LAYER) * gfull[0] + gfull[1]).astype(BF16)

    def x_half(off, half):
        return xbuf.at[pl.ds(pl.multiple_of(at_y(off) * QUART, QUART), QUART), pl.ds(half * (D // 2), D // 2)]

    def send_x(off, half, i, way):
        send(x_half(off, half), x_half(off, half), M["G"] + i, dev_y(way))

    for i, half, way in ((0, 0, 1), (2, 1, -1), (1, 1, 1), (3, 0, -1)):
        send_x(0, half, i, way)
    slots_round(4)
    relay(5)
    arrived(x_half(-1, 0), M["G"])
    send_x(-1, 0, 4, 1)
    arrived(x_half(1, 1), M["G"] + 2)
    send_x(1, 1, 5, -1)
    rows_round(2, 3, 2)
    relay(6)
    across(0)
    across(1)
    rows_round(3, 0)
    across(2)
    rows_round(3, 1)
    across(3)
    relay(7)
    rows_round(3, 3, 2)
    for i, off, half in ((1, -1, 1), (3, 1, 0), (4, 2, 0), (5, 2, 1)):
        arrived(x_half(off, half), M["G"] + i)

    hres[...] = DEEP_ALPHA * xbuf[:, my_cols].astype(F32)

    def gate_up(u):
        zu = zz(u)
        features = xbuf[:, pl.ds(pl.multiple_of(zu * 256, 256), 256)]
        for n in range(GU // 256):
            cols = slice(n * 256, (n + 1) * 256)
            part = dot(features, wbuf[zu, :, :, :, cols].reshape(256, 256), ((1,), (0,)))
            gbuf[:, cols] = part if isinstance(u, int) else gbuf[:, cols] + part

    def partner_rows(u):
        arrived(wbuf.at[zz(u), :, 1 - c, :, A_COLS], M["PA"] + u)

    partner_block(0)
    partner_rows(0)
    gate_up(0)

    def block(u, carry):
        @pl.when(u <= 3)
        def _():
            across(u + 3)

        on_step(u, 4, lambda: across(7))
        on_step(u, 5, lambda: rows_round(4, 0, 1, 3, 2))

        partner_block(u)
        partner_rows(u)
        gate_up(u)
        return carry

    lax.fori_loop(1, NZ, block, 0)
    gate = gbuf[:, 0:FH]
    hid[...] = (gate / (1.0 + jnp.exp(-gate)) * gbuf[:, FH:GU]).astype(BF16)

    def feed(off):
        return dot(hid[...], wbuf[pl.ds(at_y(off) * 2, 2), :, :, :, GU:WT].reshape(DW, FH), ((1,), (1,)))

    first, second = slice(0, HALF), slice(HALF, ROWS)
    fsend[1] = feed(2).astype(BF16)
    send(fsend.at[1, first], fthru.at[0], M["F"], dev_y(1))
    send(fsend.at[1, second], fthru.at[1], M["F"] + 1, dev_y(-1))
    after = feed(1)
    fsend[0, second] = after[second].astype(BF16)
    send(fsend.at[0, second], frecv.at[0, second], M["F"] + 2, dev_y(1))
    fkeep[0] = after[first]
    before = feed(3)
    fsend[2, first] = before[first].astype(BF16)
    send(fsend.at[2, first], frecv.at[1, first], M["F"] + 3, dev_y(-1))
    fkeep[1] = before[second]
    arrived(fthru.at[0], M["F"])
    fsend[0, first] = (fkeep[0] + fthru[0].astype(F32)).astype(BF16)
    send(fsend.at[0, first], frecv.at[0, first], M["F"] + 4, dev_y(1))
    arrived(fthru.at[1], M["F"] + 1)
    fsend[2, second] = (fkeep[1] + fthru[1].astype(F32)).astype(BF16)
    send(fsend.at[2, second], frecv.at[1, second], M["F"] + 5, dev_y(-1))
    for j in range(1, NX):
        sent(qbuf.at[0, 0:96, :], M["Q"] + (j - 1) * 2)
        sent(qbuf.at[0, 224:384, :], M["Q"] + (j - 1) * 2 + 1)
        sent(a_slot(0, 0), M["A1"] + j)
        sent(osend.at[0], M["O"] + j)
        sent(ml.at[0], M["OS"] + j)
        sent(wo.at[0, 0:V_A, wo_half(0)], M["WO"] + (j - 1) * 2)
        sent(wo.at[0, V_A:VD, wo_half(0)], M["WO"] + (j - 1) * 2 + 1)
        sent(wo.at[0, :, wo_half(0)], M["WP"] + j)
        sent(resq.at[:, my_cols], M["RS"] + j)
        sent(g1_ref, M["GN"] + j)
        sent(b1_ref, M["GN"] + 4 + j)
        sent(att.at[0], M["AT"] + j)
    for d in range(1, 5):
        for way in "MP":
            for r in range(4):
                if d < 4 or (r >= 2) == (way == "M"):
                    sent(a_slot(0, 0), M["A" + way] + 4 * d + r)
            if d < 4 or way == "M":
                sent(b_slot(0, 0), M["B" + way] + d)
    for u in range(NZ):
        sent(kvbuf.at[0, 0], M["KT"] + u)
        if u > 0:
            sent(kvbuf.at[0, 0, 0], M["KM"] + u if u < 5 else M["KP"] + u - 4)
            for j in range(1, NY):
                sent(kvbuf.at[0, 0, 0], M["KY"] + 3 * u + j - 1)
        sent(a_row(0), M["PA"] + u)
        for way in range(4):
            sent(b_slot(0, 0), M["PB"] + 4 * u + way)
        for name in ("XP", "XM"):
            sent(b_slot(0, 0), M[name] + u)
        sent(part(u, 0, 0, 0), M["RL"] + u)
    sent(part(7, 0, 0, 1), M["RL"] + 8)
    for i in range(6):
        sent(x_half(0, 0), M["G"] + i)
    hres[...] += feed(0)
    for i, k, rows in ((2, 0, second), (3, 1, first), (4, 0, first), (5, 1, second)):
        arrived(frecv.at[k, rows], M["F"] + i)
    hres[...] += frecv[0].astype(F32) + frecv[1].astype(F32)
    out_ref[...] = norm(st2, sr2, M["S2"], g2_ref, b2_ref)

    for j in range(1, NX):
        sent(st2, M["S2"] + j)
    for i in range(6):
        sent(fsend.at[0, 0:HALF], M["F"] + i)


def body(
    residual, query_latent, shared_latent, rotary_key, query_gain, latent_gain, query_narrow, key_narrow,
    value_narrow, query_wide, key_wide, value_wide, output_narrow, output_wide, first_gain, first_bias,
    gate_weight, up_weight, down_weight, second_gain, second_bias,
):
    row = lambda v: v.reshape(1, -1)
    large = (
        residual, query_latent, shared_latent, rotary_key.T, query_narrow.T, key_narrow.T, value_narrow.T,
        query_wide.T, key_wide, value_wide, output_narrow, output_wide, gate_weight, up_weight, down_weight.T,
    )
    small = (
        row(query_gain), row(latent_gain), row(first_gain), row(first_bias), row(second_gain), row(second_bias),
    )
    vmem = pl.BlockSpec(memory_space=pltpu.VMEM)
    return pl.pallas_call(
        layer_kernel,
        out_shape=jax.ShapeDtypeStruct((ROWS, DW), BF16),
        in_specs=[pl.BlockSpec(memory_space=pl.ANY)] * len(large) + [vmem] * len(small),
        out_specs=vmem,
        scratch_shapes=[
            *[pltpu.VMEM(v.shape, v.dtype) for v in large[1:10]],
            pltpu.VMEM((NZ, 2, NY, 80, LAT), BF16),
            pltpu.VMEM((NX, KX, ROWS), BF16),
            pltpu.VMEM((NZ, NX, 2, SLOT, WT), BF16),
            pltpu.VMEM((LAT, 256), BF16),
            pltpu.VMEM((VD, LAT), BF16),
            pltpu.VMEM((2 * ROWS, KX), BF16),
            pltpu.VMEM((VD, 2 * ROWS), BF16),
            pltpu.VMEM((NX, 8, ROWS), F32),
            pltpu.VMEM((NX, VD, ROWS), F32),
            pltpu.VMEM((NX, VD, ROWS), BF16),
            pltpu.VMEM((3, VD, ROWS), BF16),
            pltpu.VMEM((3, 8, ROWS), F32),
            pltpu.VMEM((VD, ROWS), F32),
            pltpu.VMEM((NY, QUART, VD), BF16),
            pltpu.VMEM((NY, QUART, VD), BF16),
            pltpu.VMEM((NY, VD, D), BF16),
            pltpu.VMEM((QUART, D), BF16),
            pltpu.VMEM((2, 1, D), F32),
            pltpu.VMEM((8, ROWS), F32),
            pltpu.VMEM((3, 8, ROWS), F32),
            pltpu.VMEM((ROWS, D), BF16),
            pltpu.VMEM((ROWS, GU), F32),
            pltpu.VMEM((ROWS, FH), BF16),
            pltpu.VMEM((3, ROWS, DW), BF16),
            pltpu.VMEM((2, ROWS, DW), BF16),
            pltpu.VMEM((2, HALF, DW), BF16),
            pltpu.VMEM((2, HALF, DW), F32),
            pltpu.VMEM((ROWS, DW), F32),
            pltpu.SemaphoreType.DMA((MESSAGES,)),
            pltpu.SemaphoreType.DMA((MESSAGES,)),
            pltpu.SemaphoreType.DMA((len(large) + 2,)),
        ],
        compiler_params=pltpu.CompilerParams(
            collective_id=0, has_side_effects=True, vmem_limit_bytes=60 * 1024 * 1024
        ),
    )(*large, *small)


def solution(mesh):
    return jax.shard_map(
        body,
        mesh=mesh,
        in_specs=(
            P("sp", "tp"),
            P("sp", None),
            P("sp", None),
            P("sp", None),
            P(),
            P(),
            P(None, "tp"),
            P(None, "tp"),
            P(None, "tp"),
            P(None, "tp"),
            P(None, "tp"),
            P(None, "tp"),
            P("tp", None),
            P("tp", None),
            P("tp"),
            P("tp"),
            P("sp", "tp"),
            P("sp", "tp"),
            P("tp", "sp"),
            P("tp"),
            P("tp"),
        ),
        out_specs=P("sp", "tp"),
        check_vma=False,
    )
```
